128 devices in a mesh: sp: 16 (over z, x), dp: 8 (over y, core).
Axes of the slice: x: 4, y: 4, z: 4, core: 2. Of those that a mesh axis runs over, the one named last changes fastest.
Arguments:
- queries: bfloat16 [8, 2048, 2048], P('dp', 'sp'), may hold values from -6 to 6
- forget_pre: bfloat16 [8, 2048, 2048], P('dp', 'sp'), may hold values from -5.5 to 5.5
- values: bfloat16 [8, 2048, 2048], P('dp', 'sp'), may hold values from -6 to 6
- out_gate: bfloat16 [8, 2048, 2048], P('dp', 'sp'), may hold values from -6 to 6
- lower_bound: float32 [2048], P('sp'), may hold values from 0.9 to 1, as said below
- head_gain: float32 [128], replicated, may hold values from 0.1 to 1.9
- residual: bfloat16 [8, 2048, 4096], P('dp', 'sp'), may hold values from -6 to 6
- out_weight: bfloat16 [2048, 4096], P(None, 'dp'), may hold values from -0.125 to 0.125
- ffn_gain: float32 [4096], replicated, may hold values from 0.1 to 1.9
- routing: int32 [8, 2048, 4], P('dp', 'sp'), may hold values from 0 to 127, all different within a row; in each aligned block of 128 rows (0 to 127, 128 to 255, ..., all dimensions but the last counted through in order) at most 5 rows name the same one
- route_weight: float32 [8, 2048, 4], P('dp', 'sp'), may hold values from 0.1 to 1
- expert_gate: bfloat16 [128, 4096, 512], P(('sp', 'dp')), may hold values from -0.09375 to 0.09375
- expert_up: bfloat16 [128, 4096, 512], P(('sp', 'dp')), may hold values from -0.09375 to 0.09375
- expert_down: bfloat16 [128, 512, 4096], P(('sp', 'dp')), may hold values from -0.25 to 0.25
Outputs:
- layer_out: bfloat16 [8, 2048, 4096], P('dp', 'sp')
The draws below stay inside these ranges and needn't reach their ends.
Inputs may be any that keep to these rules, and one draw needn't show every extreme that they name: `routing`: within the rows of one device no expert is named more than 5 times, and in some devices one is named exactly 5 times; the 4 experts of a row differ. `lower_bound`: every entry is below 1.
All inputs are finite; a program needn't handle non-finite values.
Results may differ from the reference program's by a relative error of at most 0.0073.
Values may be sent and summed in bfloat16 or wider, within the bound.
No kernel may reach another device: no remote copies, remote signals or barrier semaphores. Data moves between devices by JAX's collectives and lax.ppermute only.
A program may use at most 128 MiB of HBM per device.

```python
import math
import jax
import jax.numpy as jnp
import numpy as np
from jax import lax

D = 4096
HEADS = 16
HEAD_DIM = 128
A_WIDTH = 2048
FE = 512
EXPERTS = 128
TOP_K = 4
BLOCK = 128
TOK_DEV = 128
SEQLEN = 2048
CAP = 5
N_DP = 8


def draw_forget_pre(key, part):
    noise_key = jax.random.fold_in(key, 11)
    shift_key = jax.random.fold_in(key, 12)
    noise = jax.random.truncated_normal(noise_key, -4.0, 4.0, (N_DP, SEQLEN, A_WIDTH), jnp.float32)
    block_shift = jax.random.uniform(shift_key, (N_DP, SEQLEN // TOK_DEV, 1, 1), jnp.float32, -1.5, 1.5)
    noise = noise.reshape(N_DP, SEQLEN // TOK_DEV, TOK_DEV, A_WIDTH) + block_shift
    return noise.reshape(N_DP, SEQLEN, A_WIDTH).astype(jnp.bfloat16)


def draw_lower_bound(key, part):
    pick_key = jax.random.fold_in(key, 21)
    unit_key = jax.random.fold_in(key, 22)
    fast_heads = jax.random.randint(pick_key, (HEADS, 1), 0, 16) < 8
    unit_draw = jax.random.uniform(unit_key, (HEADS, HEAD_DIM), jnp.float32)
    slow_rate = 0.3 / SEQLEN * (20.0 / 3.0) ** unit_draw
    fast_rate = 1.0 / 50.0 * (50.0 / 15.0) ** unit_draw
    leak_rate = jnp.where(fast_heads, fast_rate, slow_rate)
    return (1.0 - leak_rate).reshape(A_WIDTH).astype(jnp.float32)


def shard_levels(own_key, shape, shards, low, high):
    def one(position, parts):
        steps = jax.random.uniform(jax.random.fold_in(jax.random.fold_in(own_key, 6), position), (parts,), jnp.float32, low / len(shards), high / len(shards))
        return jnp.repeat(jnp.exp(steps), shape[position] // parts).reshape((-1,) + (1,) * (len(shape) - position - 1))

    loudness = one(*shards[0])
    for cut in shards[1:]:
        loudness = loudness * one(*cut)
    return loudness


def shared_out(rng, own, number, rows, amount, top, most, skew):
    sequence = jax.random.permutation(rng, amount)
    crowded, usual = load_shares(amount, rows * top, most, skew, True), load_shares(amount, rows * top, most, skew, False)
    places = jnp.arange(amount)

    def named(tallies, rotation):
        used = int((tallies > 0).sum())
        fixed = max(1, used // 4)
        moved = fixed + (places - fixed + rotation * (used - fixed)) % max(1, amount - fixed)
        return jnp.zeros((amount,), jnp.int32).at[sequence[jnp.where(places < fixed, places, moved)]].set(jnp.asarray(tallies, jnp.int32))

    tallies = jnp.where(number % 4 == 0, named(crowded, number // 4), named(usual, number - number // 4 - 1))
    mixed = jax.random.permutation(jax.random.fold_in(own, 3), amount)
    source_of, sink = mixed[0:amount // 2 * 2:2], mixed[1:amount // 2 * 2:2]
    margin = jnp.minimum(tallies[source_of] - 1, most - tallies[sink]) // 2
    margin = jnp.where((source_of == sequence[0]) | (sink == sequence[0]) | (tallies[sink] == 0), 0, jnp.maximum(margin, 0))
    moved = jax.random.randint(jax.random.fold_in(own, 4), (amount // 2,), 0, 1 << 20) % (margin + 1)
    tallies = tallies.at[source_of].add(-moved).at[sink].add(moved)
    items = jnp.searchsorted(jnp.cumsum(tallies), jnp.arange(rows * top), side="right").astype(jnp.int32)
    table = items.reshape(top, rows).T
    table = table[jax.random.permutation(jax.random.fold_in(own, 1), rows)]
    rotation = jax.random.randint(jax.random.fold_in(own, 2), (rows, 1), 0, top)
    return jnp.take_along_axis(table, (jnp.arange(top)[None, :] + rotation) % top, axis=1)


def load_shares(number_of, total, limit, lean, full):
    portions = [(1 << 20) // math.isqrt(standing ** lean) + 1 for standing in range(1, number_of + 1)]
    largest = limit if full else min(limit, max(-(-total // number_of), total * portions[0] // sum(portions)))
    least = 1 if total - largest >= number_of - 1 else 0
    given, rest = [largest] + [least] * (number_of - 1), total - largest - least * (number_of - 1)
    while rest > 0:
        candidates = [i for i in range(1, number_of) if given[i] < largest] or [i for i in range(1, number_of) if given[i] < limit]
        mass, budget = sum([portions[i] for i in candidates]), rest
        for i in candidates:
            extra = min(limit - given[i], max(1, budget * portions[i] // mass), rest)
            given[i] = given[i] + extra
            rest = rest - extra
    return np.array(given)


def normal_values(stream_key, dims, scale, limit, pieces=(), kind=jnp.bfloat16):
    factor_of = shard_levels(stream_key, dims, pieces, -0.22, 0.18) if pieces else 1.0
    drawn = jax.random.normal(stream_key, dims, jnp.float32) * scale * factor_of
    return jnp.minimum(jnp.maximum(drawn, -limit), limit).astype(kind)


def setup_inputs(seed: int = 0) -> dict:
    keys = jax.random.split(jax.random.key(seed), 15)
    queries = normal_values(keys[0], (N_DP, SEQLEN, A_WIDTH), 1.0, 6.0, ((0, 8), (1, 16)))
    forget_pre = draw_forget_pre(jax.random.fold_in(keys[14], 71), 0)
    values = normal_values(keys[2], (N_DP, SEQLEN, A_WIDTH), 1.0, 6.0, ((0, 8), (1, 16)))
    out_gate = normal_values(keys[3], (N_DP, SEQLEN, A_WIDTH), 1.0, 6.0, ((0, 8), (1, 16)))
    lower_bound = draw_lower_bound(jax.random.fold_in(keys[14], 71), 0)
    head_gain = jnp.clip(1.0 + 0.18 * jax.random.normal(keys[5], (HEAD_DIM,), jnp.float32), 0.1, 1.9)
    residual = normal_values(keys[6], (N_DP, SEQLEN, D), 1.0, 6.0, ((0, 8), (1, 16)))
    out_weight = normal_values(keys[7], (A_WIDTH, D), A_WIDTH ** -0.5, 0.125, ((1, 8),))
    ffn_gain = jnp.clip(1.0 + 0.18 * jax.random.normal(keys[8], (D,), jnp.float32), 0.1, 1.9)
    routing_keys = jax.random.split(jax.random.fold_in(keys[9], 1), N_DP * SEQLEN // TOK_DEV)
    routing_turns = jax.random.permutation(jax.random.fold_in(keys[9], 3), N_DP * SEQLEN // TOK_DEV)
    routing = jax.vmap(lambda own, number: shared_out(jax.random.fold_in(keys[9], 2), own, number, TOK_DEV, EXPERTS, TOP_K, CAP, 2))(routing_keys, routing_turns).reshape((N_DP, SEQLEN, TOP_K))
    route_weight = jnp.clip(0.1 + 0.9 * jax.random.uniform(keys[10], (N_DP, SEQLEN, TOP_K), jnp.float32) ** shard_levels(keys[10], (N_DP, SEQLEN, TOP_K), ((0, 8), (1, 16)), -0.2, 0.2), 0.1, 1.0)
    expert_gate = normal_values(keys[11], (EXPERTS, D, FE), D ** -0.5, 0.09375, ((0, 128),))
    expert_up = normal_values(keys[12], (EXPERTS, D, FE), D ** -0.5, 0.09375, ((0, 128),))
    expert_down = normal_values(keys[13], (EXPERTS, FE, D), FE ** -0.5, 0.25, ((0, 128),))
    return dict(queries=queries, forget_pre=forget_pre, values=values, out_gate=out_gate, lower_bound=lower_bound, head_gain=head_gain, residual=residual, out_weight=out_weight, ffn_gain=ffn_gain, routing=routing, route_weight=route_weight, expert_gate=expert_gate, expert_up=expert_up, expert_down=expert_down)


PRECISE = lax.Precision.HIGHEST
NORM_EPS = 1e-06

def block_recurrence(query_f, log_keep, key_f, value_f):
    log_run = jnp.cumsum(log_keep, axis=1)
    log_last = log_run[:, -1]
    q_scaled = query_f * jnp.exp(log_run)
    k_scaled = key_f * jnp.exp(-log_run)
    k_carry = key_f * jnp.exp(log_last[:, None] - log_run)
    causal = jnp.tril(jnp.ones((BLOCK, BLOCK), bool))
    scores = jnp.einsum('nthk,nshk->nhts', q_scaled, k_scaled, precision=PRECISE)
    scores = jnp.where(causal, scores, 0.0)
    within = jnp.einsum('nhts,nshv->nthv', scores, value_f, precision=PRECISE)
    push_state = jnp.einsum('nshk,nshv->nhkv', k_carry, value_f, precision=PRECISE)
    keep_block = jnp.exp(log_last)

    def advance(state_now, block_item):
        keep_now, push_now = block_item
        return (keep_now[..., None] * state_now + push_now, state_now)
    start_state = jnp.zeros(push_state.shape[1:], jnp.float32)
    _, before = lax.scan(advance, start_state, (keep_block, push_state))
    carried = jnp.einsum('nthk,nhkv->nthv', q_scaled, before, precision=PRECISE)
    return within + carried

def reference(queries, forget_pre, values, out_gate, lower_bound, head_gain, residual, out_weight, ffn_gain, routing, route_weight, expert_gate, expert_up, expert_down):
    leak_rate = (1.0 - lower_bound) * jax.nn.sigmoid(-forget_pre.astype(jnp.float32))
    log_keep = jnp.log1p(-leak_rate)
    layout = (N_DP, SEQLEN // BLOCK, BLOCK, HEADS, HEAD_DIM)

    def one_sequence(seq_item):
        return block_recurrence(seq_item[0], seq_item[1], seq_item[2], seq_item[3])
    mix = lax.map(one_sequence, (queries.astype(jnp.float32).reshape(layout), log_keep.reshape(layout), leak_rate.reshape(layout), values.astype(jnp.float32).reshape(layout)))
    scale = lax.rsqrt(lax.optimization_barrier(jnp.mean(mix * mix, axis=-1, keepdims=True)) + NORM_EPS)
    normed = (mix * scale * head_gain).astype(jnp.bfloat16).reshape(N_DP * SEQLEN, A_WIDTH)
    gated_out = (normed.astype(jnp.float32) * jax.nn.silu(out_gate.reshape(N_DP * SEQLEN, A_WIDTH).astype(jnp.float32))).astype(jnp.bfloat16)
    projected = jnp.dot(gated_out, out_weight, preferred_element_type=jnp.float32).astype(jnp.bfloat16)
    hidden = (residual.reshape(N_DP * SEQLEN, D).astype(jnp.float32) + projected.astype(jnp.float32)).astype(jnp.bfloat16)
    hidden_f = hidden.astype(jnp.float32)
    moe_in = (hidden_f * lax.rsqrt(lax.optimization_barrier(jnp.mean(hidden_f * hidden_f, axis=-1, keepdims=True)) + NORM_EPS) * ffn_gain).astype(jnp.bfloat16)
    all_rows = N_DP * SEQLEN
    blocks = all_rows // TOK_DEV
    per_expert = blocks * CAP
    chosen = routing.reshape(blocks, TOK_DEV * TOP_K).astype(jnp.int32)
    matches = (chosen[:, :, None] == jnp.arange(EXPERTS, dtype=jnp.int32)[None, None, :]).astype(jnp.int32)
    rank_in = lax.optimization_barrier(jnp.sum((jnp.cumsum(matches, axis=1) - 1) * matches, axis=2)).astype(jnp.int32)
    target = chosen * per_expert + jnp.arange(blocks, dtype=jnp.int32)[:, None] * CAP + rank_in
    target = target.reshape(-1).astype(jnp.int32)
    owners = jnp.arange(all_rows * TOP_K, dtype=jnp.int32) // TOP_K
    slot_owner = jnp.full((EXPERTS * per_expert,), all_rows, jnp.int32).at[target].set(owners)
    slot_weight = jnp.zeros((EXPERTS * per_expert,), jnp.float32).at[target].set(route_weight.reshape(-1))
    padded = jnp.concatenate([moe_in, jnp.zeros((1, D), jnp.bfloat16)], axis=0)

    def add_expert(weighted, expert_item):
        owner_rows, weight_rows, w_gate, w_up, w_down = expert_item
        slot_rows = padded[owner_rows]
        gate_part = jnp.dot(slot_rows, w_gate, preferred_element_type=jnp.float32)
        up_part = jnp.dot(slot_rows, w_up, preferred_element_type=jnp.float32)
        act = (jax.nn.silu(gate_part) * up_part).astype(jnp.bfloat16)
        expert_out = jnp.dot(act, w_down, preferred_element_type=jnp.float32).astype(jnp.bfloat16)
        return (weighted.at[owner_rows].add(expert_out.astype(jnp.float32) * weight_rows[:, None]), None)
    weighted, _ = lax.scan(add_expert, jnp.zeros((all_rows + 1, D), jnp.float32), (slot_owner.reshape(EXPERTS, per_expert), slot_weight.reshape(EXPERTS, per_expert), expert_gate, expert_up, expert_down))
    layer_out = (hidden_f + weighted[:all_rows]).astype(jnp.bfloat16)
    return layer_out.reshape(N_DP, SEQLEN, D)
```

```python
import functools

import jax
import jax.numpy as jnp
from jax import lax
from jax.experimental import pallas as pl
from jax.experimental.pallas import tpu as pltpu
from jax.sharding import PartitionSpec as P

NORM_EPS = 1e-06
LANES = 128
CAPACITY = 5
BF16 = jnp.bfloat16
F32 = jnp.float32
MSG_PAD = 16


def dot(a, b, dims=((1,), (0,)), precision=None):
    return lax.dot_general(
        a, b, (dims, ((), ())), preferred_element_type=F32, precision=precision
    )


def gate_terms(forget_ref, bound_ref):
    leak = (1.0 - bound_ref[...]) * jax.nn.sigmoid(-forget_ref[...].astype(F32))
    log_keep = jnp.log1p(-leak)
    rows = log_keep.shape[0]
    at = lax.broadcasted_iota(jnp.int32, (rows, rows), 0)
    of = lax.broadcasted_iota(jnp.int32, (rows, rows), 1)
    causal = of <= at
    log_run = dot(jnp.where(causal, 1.0, 0.0), log_keep, precision=lax.Precision.HIGHEST)
    return leak, log_run, causal


def push_kernel(forget_ref, value_ref, bound_ref, message_ref):
    leak, log_run, _ = gate_terms(forget_ref, bound_ref)
    rows, size = leak.shape
    log_last = log_run[rows - 1 : rows, :]
    carry = leak * jnp.exp(log_last - log_run)
    push = dot(value_ref[...], carry.astype(BF16), ((0,), (0,)))
    message_ref[0, 0:size, :] = push.astype(BF16)
    keep = jnp.exp(log_last)
    high = keep.astype(BF16)
    low = (keep - high.astype(F32)).astype(BF16)
    row = lax.broadcasted_iota(jnp.int32, (MSG_PAD, size), 0)
    tail = jnp.where(row == 0, high.astype(F32), jnp.where(row == 1, low.astype(F32), 0.0))
    message_ref[0, size : size + MSG_PAD, :] = tail.astype(BF16)


def scan_kernel(message_ref, before_ref):
    blocks, _, size = message_ref.shape
    state = jnp.zeros((size, size), F32)
    for n in range(blocks):
        before_ref[n] = state.astype(BF16)
        tail = message_ref[n, size : size + MSG_PAD, :].astype(F32)
        keep = tail[0:1, :] + tail[1:2, :]
        state = keep * state + message_ref[n, 0:size, :].astype(F32)


def mix_kernel(
    query_ref, forget_ref, value_ref, gate_ref, bound_ref, before_ref, gain_ref, out_ref
):
    leak, log_run, causal = gate_terms(forget_ref, bound_ref)
    q_scaled = (query_ref[...].astype(F32) * jnp.exp(log_run)).astype(BF16)
    k_scaled = (leak * jnp.exp(-log_run)).astype(BF16)
    scores = jnp.where(causal, dot(q_scaled, k_scaled, ((1,), (1,))), 0.0)
    mix = dot(scores.astype(BF16), value_ref[...])
    mix = mix + dot(q_scaled, before_ref[0], ((1,), (1,)))
    scale = lax.rsqrt(jnp.mean(mix * mix, axis=-1, keepdims=True) + NORM_EPS)
    normed = (mix * scale * gain_ref[...]).astype(BF16)
    u = gate_ref[...].astype(F32)
    out_ref[...] = (normed.astype(F32) * (u / (1.0 + jnp.exp(-u)))).astype(BF16)


def project_kernel(
    slot_ref,
    gated_ref,
    weight_ref,
    residual_ref,
    gain_ref,
    outgoing_ref,
    hidden_ref,
    wide_ref,
    square_ref,
    moe_ref,
    keep_ref,
):
    step = pl.program_id(0)
    tokens, columns = residual_ref.shape
    width = wide_ref.shape[1]
    pieces = width // LANES
    projected = dot(gated_ref[...], weight_ref[0]).astype(BF16)
    hidden = (residual_ref[...].astype(F32) + projected.astype(F32)).astype(BF16).astype(F32)
    at = pl.multiple_of(step * columns, columns)
    wide_ref[:, pl.ds(at, columns)] = hidden
    squares = jnp.sum(hidden * hidden, axis=-1, keepdims=True)

    @pl.when(step == 0)
    def _():
        square_ref[...] = jnp.zeros_like(square_ref)

    square_ref[...] += jnp.broadcast_to(squares, square_ref.shape)

    @pl.when(step == pl.num_programs(0) - 1)
    def _():
        scale = lax.rsqrt(square_ref[...] / width + NORM_EPS)
        for c in range(pieces):
            part = wide_ref[:, c * LANES : (c + 1) * LANES]
            keep_ref[pl.ds(c, tokens, stride=pieces), :] = part
            gain = gain_ref[:, c * LANES : (c + 1) * LANES]
            moe_ref[pl.ds(c, tokens, stride=pieces), :] = part * scale * gain

        def keep_row(t, _):
            row = pl.multiple_of(t * pieces, pieces)
            hidden_ref[t] = keep_ref[pl.ds(row, pieces), :].astype(BF16)
            return 0

        lax.fori_loop(0, tokens, keep_row, 0, unroll=4)

        def fill_slot(s, _):
            row = pl.multiple_of(slot_ref[s] * pieces, pieces)
            outgoing_ref[s] = moe_ref[pl.ds(row, pieces), :].astype(BF16)
            return 0

        lax.fori_loop(0, outgoing_ref.shape[0], fill_slot, 0, unroll=8)


def expert_kernel(rows_ref, gate_ref, up_ref, down_ref, out_ref, wide_ref, x_ref):
    rows, pieces, _ = rows_ref.shape
    wide_ref[...] = rows_ref[...].astype(F32).reshape(rows * pieces, LANES)
    for c in range(pieces):
        x_ref[:, c * LANES : (c + 1) * LANES] = wide_ref[
            pl.ds(c, rows, stride=pieces), :
        ].astype(BF16)
    x = x_ref[...]
    gate = dot(x, gate_ref[0])
    up = dot(x, up_ref[0])
    act = (gate / (1.0 + jnp.exp(-gate)) * up).astype(BF16)
    for c in range(pieces):
        part = dot(act, down_ref[0, :, c * LANES : (c + 1) * LANES])
        wide_ref[pl.ds(c, rows, stride=pieces), :] = part
    out_ref[...] = wide_ref[...].reshape(rows, pieces, LANES).astype(BF16)


def combine_kernel(target_ref, weight_ref, back_ref, hidden_ref, out_ref, wide_ref):
    tokens, pieces, _ = hidden_ref.shape
    top = target_ref.shape[0] // tokens

    def one(t, _):
        total = jnp.zeros((pieces, LANES), F32)
        for j in range(top):
            i = t * top + j
            total = total + weight_ref[i] * back_ref[target_ref[i]].astype(F32)
        row = pl.multiple_of(t * pieces, pieces)
        wide_ref[pl.ds(row, pieces), :] = hidden_ref[t].astype(F32) + total
        return 0

    lax.fori_loop(0, tokens, one, 0, unroll=4)
    for c in range(pieces):
        out_ref[:, c * LANES : (c + 1) * LANES] = wide_ref[
            pl.ds(c, tokens, stride=pieces), :
        ].astype(BF16)


def whole(shape, space=None):
    if space is None:
        return pl.BlockSpec(shape, lambda *_: (0,) * len(shape))
    return pl.BlockSpec(memory_space=space)


def cost(flops, moved):
    return pl.CostEstimate(flops=int(flops), bytes_accessed=int(moved), transcendentals=0)


def slots_of(chosen, experts, capacity, tokens, top_count):
    matches = (chosen[:, None] == jnp.arange(experts, dtype=jnp.int32)[None, :]).astype(jnp.int32)
    rank_in = jnp.sum((jnp.cumsum(matches, axis=0) - 1) * matches, axis=1)
    target = chosen * capacity + rank_in
    owners = jnp.arange(tokens * top_count, dtype=jnp.int32) // top_count
    slot_owner = jnp.zeros((experts * capacity,), jnp.int32).at[target].set(owners)
    return target, slot_owner


def local(
    queries,
    forget_pre,
    values,
    out_gate,
    lower_bound,
    head_gain,
    residual,
    out_weight,
    ffn_gain,
    routing,
    route_weight,
    expert_gate,
    expert_up,
    expert_down,
):
    tokens = queries.shape[1]
    channels = queries.shape[2]
    size = head_gain.shape[0]
    heads = channels // size
    width = residual.shape[2]
    pieces = width // LANES
    top_count = routing.shape[2]
    span = lax.axis_size("sp") * lax.axis_size("dp")
    experts = expert_gate.shape[0] * span
    slots = experts * CAPACITY

    weights_all = lax.all_gather(out_weight, "dp")
    bound = lax.all_gather(lower_bound, "sp", tiled=True).reshape(1, channels)
    target, slot_owner = slots_of(
        routing.reshape(tokens * top_count), experts, CAPACITY, tokens, top_count
    )

    head_block = pl.BlockSpec((tokens, size), lambda h: (0, h))
    bound_block = pl.BlockSpec((1, size), lambda h: (0, h))
    q = queries.reshape(tokens, channels)
    f = forget_pre.reshape(tokens, channels)
    v = values.reshape(tokens, channels)
    g = out_gate.reshape(tokens, channels)
    message = pl.pallas_call(
        push_kernel,
        grid=(heads,),
        in_specs=[head_block, head_block, bound_block],
        out_specs=pl.BlockSpec((1, size + MSG_PAD, size), lambda h: (h, 0, 0)),
        out_shape=jax.ShapeDtypeStruct((heads, size + MSG_PAD, size), BF16),
        cost_estimate=cost(8e8, 2e6),
        name="push",
    )(f, v, bound)
    arrived = lax.all_to_all(message, "sp", split_axis=0, concat_axis=0, tiled=True)
    before = pl.pallas_call(
        scan_kernel,
        out_shape=jax.ShapeDtypeStruct((arrived.shape[0], size, size), BF16),
        cost_estimate=cost(1e8, 1e6),
        name="scan",
    )(arrived)
    before = lax.all_to_all(before, "sp", split_axis=0, concat_axis=0, tiled=True)
    gated = pl.pallas_call(
        mix_kernel,
        grid=(heads,),
        in_specs=[head_block] * 4
        + [
            bound_block,
            pl.BlockSpec((1, size, size), lambda h: (h, 0, 0)),
            pl.BlockSpec((1, size), lambda h: (0, 0)),
        ],
        out_specs=head_block,
        out_shape=jax.ShapeDtypeStruct((tokens, channels), BF16),
        cost_estimate=cost(1.2e9, 3e6),
        name="mix",
    )(q, f, v, g, bound, before, head_gain.reshape(1, size))

    columns = out_weight.shape[1]
    outgoing, hidden = pl.pallas_call(
        project_kernel,
        grid=(width // columns,),
        in_specs=[
            whole(None, pltpu.SMEM),
            pl.BlockSpec((tokens, channels), lambda i: (0, 0)),
            pl.BlockSpec((1, channels, columns), lambda i: (i, 0, 0)),
            pl.BlockSpec((tokens, columns), lambda i: (0, i)),
            pl.BlockSpec((1, width), lambda i: (0, 0)),
        ],
        out_specs=[
            pl.BlockSpec((slots, pieces, LANES), lambda i: (0, 0, 0)),
            pl.BlockSpec((tokens, pieces, LANES), lambda i: (0, 0, 0)),
        ],
        out_shape=[
            jax.ShapeDtypeStruct((slots, pieces, LANES), BF16),
            jax.ShapeDtypeStruct((tokens, pieces, LANES), BF16),
        ],
        scratch_shapes=[
            pltpu.VMEM((tokens, width), F32),
            pltpu.VMEM((tokens, LANES), F32),
            pltpu.VMEM((tokens * pieces, LANES), F32),
            pltpu.VMEM((tokens * pieces, LANES), F32),
        ],
        cost_estimate=cost(2.2e9, 24e6),
        compiler_params=pltpu.CompilerParams(vmem_limit_bytes=40 * 2**20),
        name="project",
    )(
        slot_owner,
        gated,
        weights_all,
        residual.reshape(tokens, width),
        ffn_gain.reshape(1, width),
    )

    exchange = functools.partial(
        lax.all_to_all, axis_name=("sp", "dp"), split_axis=0, concat_axis=0, tiled=True
    )
    chunk = (span, CAPACITY * pieces, LANES)
    rows_in = exchange(outgoing.reshape(chunk)).reshape(slots, pieces, LANES)
    hidden_units = expert_gate.shape[2]
    rows = tokens
    row_block = pl.BlockSpec((rows, pieces, LANES), lambda i: (i, 0, 0))
    results = pl.pallas_call(
        expert_kernel,
        grid=(slots // rows,),
        in_specs=[
            row_block,
            pl.BlockSpec((1, width, hidden_units), lambda i: (0, 0, 0)),
            pl.BlockSpec((1, width, hidden_units), lambda i: (0, 0, 0)),
            pl.BlockSpec((1, hidden_units, width), lambda i: (0, 0, 0)),
        ],
        out_specs=row_block,
        out_shape=jax.ShapeDtypeStruct((slots, pieces, LANES), BF16),
        scratch_shapes=[
            pltpu.VMEM((rows * pieces, LANES), F32),
            pltpu.VMEM((rows, width), BF16),
        ],
        cost_estimate=cost(8e9, 24e6),
        compiler_params=pltpu.CompilerParams(vmem_limit_bytes=48 * 2**20),
        name="expert",
    )(rows_in, expert_gate, expert_up, expert_down)
    back = exchange(results.reshape(chunk)).reshape(slots, pieces, LANES)
    out = pl.pallas_call(
        combine_kernel,
        in_specs=[
            whole(None, pltpu.SMEM),
            whole(None, pltpu.SMEM),
            whole(None, pltpu.VMEM),
            whole(None, pltpu.VMEM),
        ],
        out_specs=whole(None, pltpu.VMEM),
        out_shape=jax.ShapeDtypeStruct((tokens, width), BF16),
        scratch_shapes=[pltpu.VMEM((tokens * pieces, LANES), F32)],
        cost_estimate=cost(4e8, 8e6),
        compiler_params=pltpu.CompilerParams(vmem_limit_bytes=32 * 2**20),
        name="combine",
    )(target, route_weight.reshape(tokens * top_count), back, hidden)
    return out.reshape(1, tokens, width)


def solution(mesh):
    in_specs = (
        P("dp", "sp", None),
        P("dp", "sp", None),
        P("dp", "sp", None),
        P("dp", "sp", None),
        P("sp"),
        P(),
        P("dp", "sp", None),
        P(None, "dp"),
        P(),
        P("dp", "sp", None),
        P("dp", "sp", None),
        P(("sp", "dp"), None, None),
        P(("sp", "dp"), None, None),
        P(("sp", "dp"), None, None),
    )
    out_specs = P("dp", "sp", None)
    return jax.shard_map(local, mesh=mesh, in_specs=in_specs, out_specs=out_specs, check_vma=False)
```

```python
import functools

import jax
import jax.numpy as jnp
from jax import lax
from jax.experimental import pallas as pl
from jax.experimental.pallas import tpu as pltpu
from jax.sharding import PartitionSpec as P

NORM_EPS = 1e-06
LANES = 128
CAPACITY = 5
BF16 = jnp.bfloat16
F32 = jnp.float32
MSG_PAD = 16


def dot(a, b, dims=((1,), (0,)), precision=None):
    return lax.dot_general(
        a, b, (dims, ((), ())), preferred_element_type=F32, precision=precision
    )


def split(x):
    high = x.astype(BF16)
    return high, (x - high.astype(F32)).astype(BF16)


def tril(rows):
    at = lax.broadcasted_iota(jnp.int32, (rows, rows), 0)
    of = lax.broadcasted_iota(jnp.int32, (rows, rows), 1)
    return of <= at


def gate_terms(forget, free):
    leak = free * jax.nn.sigmoid(-forget.astype(F32))
    causal = jnp.where(tril(leak.shape[0]), 1.0, 0.0)
    log_run = dot(causal, jnp.log1p(-leak), precision=lax.Precision.HIGHEST)
    return leak, log_run


def pair_kernel(forget_ref, value_ref, out_ref):
    size = out_ref.shape[3]
    for h in range(out_ref.shape[0]):
        out_ref[h, 0] = forget_ref[:, h * size : (h + 1) * size]
        out_ref[h, 1] = value_ref[:, h * size : (h + 1) * size]


def state_kernel(pair_ref, bound_ref, before_ref):
    blocks, _, rows, size = pair_ref.shape
    free = 1.0 - bound_ref[...]
    high = free.astype(BF16).astype(F32)
    mid = (free - high).astype(BF16).astype(F32)
    low = free - high - mid
    row = lax.broadcasted_iota(jnp.int32, (MSG_PAD, size), 0)
    tail = jnp.where(
        row == 0, high, jnp.where(row == 1, mid, jnp.where(row == 2, low, 0.0))
    ).astype(BF16)
    group = 4

    def some(i, state):
        forget = jnp.concatenate([pair_ref[i * group + j, 0] for j in range(group)], axis=1)
        leak, log_run = gate_terms(forget, jnp.concatenate([free] * group, axis=1))
        log_last = log_run[rows - 1 : rows, :]
        carry = leak * jnp.exp(log_last - log_run)
        keep = jnp.exp(log_last)
        for j in range(group):
            n = i * group + j
            before_ref[n, 0:size, :] = state.astype(BF16)
            before_ref[n, size : size + MSG_PAD, :] = tail
            at = slice(j * size, (j + 1) * size)
            upper, lower = split(carry[:, at])
            value = pair_ref[n, 1]
            push = dot(value, upper, ((0,), (0,))) + dot(value, lower, ((0,), (0,)))
            state = keep[:, at] * state + push
        return state

    lax.fori_loop(0, blocks // group, some, jnp.zeros((size, size), F32))


def mix_kernel(query_ref, forget_ref, value_ref, gate_ref, before_ref, gain_ref, out_ref):
    heads, _, size = before_ref.shape
    tails = [before_ref[h, size : size + MSG_PAD, :].astype(F32) for h in range(heads)]
    free = jnp.concatenate([t[2:3] + t[1:2] + t[0:1] for t in tails], axis=1)
    leak, log_run = gate_terms(forget_ref[...], free)
    q_scaled = query_ref[...].astype(F32) * jnp.exp(log_run)
    k_scaled = leak * jnp.exp(-log_run)
    q_high, q_low = split(q_scaled)
    k_high, k_low = split(k_scaled)
    causal = tril(leak.shape[0])
    u = gate_ref[...].astype(F32)
    silu = u / (1.0 + jnp.exp(-u))
    lanes = ((1,), (1,))
    for h in range(heads):
        at = slice(h * size, (h + 1) * size)
        scores = (
            dot(q_high[:, at], k_high[:, at], lanes)
            + dot(q_high[:, at], k_low[:, at], lanes)
            + dot(q_low[:, at], k_high[:, at], lanes)
        )
        s_high, s_low = split(jnp.where(causal, scores, 0.0))
        value = value_ref[:, at]
        before = before_ref[h, 0:size, :]
        mix = (
            dot(s_high, value)
            + dot(s_low, value)
            + dot(q_high[:, at], before, lanes)
            + dot(q_low[:, at], before, lanes)
        )
        scale = lax.rsqrt(jnp.mean(mix * mix, axis=-1, keepdims=True) + NORM_EPS)
        normed = (mix * scale * gain_ref[...]).astype(BF16)
        out_ref[:, at] = (normed.astype(F32) * silu[:, at]).astype(BF16)


def block_products(rows_ref, refs):
    at, total = 0, None
    for w_ref in refs:
        depth = w_ref.shape[0]
        part = dot(rows_ref[:, at : at + depth], w_ref[...])
        total = part if total is None else total + part
        at += depth
        if at == rows_ref.shape[1]:
            yield total.astype(BF16)
            at, total = 0, None


def columns_kernel(mine_ref, other_ref, *refs):
    *w_refs, keep_ref, give_ref = refs
    columns = w_refs[0].shape[1]
    for src, dst in ((mine_ref, keep_ref), (other_ref, give_ref)):
        for n, block in enumerate(block_products(src, w_refs)):
            dst[:, n * columns : (n + 1) * columns] = block


def route_kernel(slot_ref, order_ref, *refs):
    *part_refs, residual_ref, gain_ref, outgoing_ref, hidden_ref, wide_ref, moe_ref, keep_ref = refs
    tokens, width = residual_ref.shape
    pieces = width // LANES
    columns = width // order_ref.shape[0]
    skew = moe_ref.shape[0] // pieces
    squares = jnp.zeros((tokens, 1), F32)
    parts = [
        ref[:, n * columns : (n + 1) * columns]
        for ref in part_refs
        for n in range(ref.shape[1] // columns)
    ]
    for n, part in enumerate(parts):
        at = pl.multiple_of(order_ref[n] * columns, columns)
        hidden = residual_ref[:, pl.ds(at, columns)].astype(F32) + part.astype(F32)
        hidden = hidden.astype(BF16).astype(F32)
        wide_ref[:, pl.ds(at, columns)] = hidden
        squares = squares + jnp.sum(hidden * hidden, axis=-1, keepdims=True)
    scale = lax.rsqrt(squares / width + NORM_EPS)
    for c in range(pieces):
        part = wide_ref[:, c * LANES : (c + 1) * LANES]
        keep_ref[c * skew : c * skew + tokens, :] = part
        gain = gain_ref[:, c * LANES : (c + 1) * LANES]
        moe_ref[c * skew : c * skew + tokens, :] = part * scale * gain

    def keep_row(t, _):
        hidden_ref[t] = keep_ref[pl.ds(t, pieces, stride=skew), :].astype(BF16)
        return 0

    lax.fori_loop(0, tokens, keep_row, 0, unroll=4)

    def fill_slot(s, _):
        outgoing_ref[s] = moe_ref[pl.ds(slot_ref[s], pieces, stride=skew), :].astype(BF16)
        return 0

    lax.fori_loop(0, outgoing_ref.shape[0], fill_slot, 0, unroll=8)


def expert_kernel(rows_ref, gate_ref, up_ref, down_ref, out_ref, wide_ref, x_ref):
    pieces = rows_ref.shape[1]
    rows = x_ref.shape[0]
    skew = wide_ref.shape[0] // pieces

    def some(i, _):
        first = i * rows

        def spread(r, _):
            wide_ref[pl.ds(r, pieces, stride=skew), :] = rows_ref[first + r].astype(F32)
            return 0

        lax.fori_loop(0, rows, spread, 0, unroll=8)
        for c in range(pieces):
            x_ref[:, c * LANES : (c + 1) * LANES] = wide_ref[
                c * skew : c * skew + rows, :
            ].astype(BF16)
        gate = dot(x_ref[...], gate_ref[...])
        up = dot(x_ref[...], up_ref[...])
        act = (gate / (1.0 + jnp.exp(-gate)) * up).astype(BF16)
        step = 4
        for c in range(0, pieces, step):
            part = dot(act, down_ref[:, c * LANES : (c + step) * LANES])
            for k in range(step):
                wide_ref[(c + k) * skew : (c + k) * skew + rows, :] = part[
                    :, k * LANES : (k + 1) * LANES
                ]

        def gather(r, _):
            out_ref[first + r] = wide_ref[pl.ds(r, pieces, stride=skew), :].astype(BF16)
            return 0

        lax.fori_loop(0, rows, gather, 0, unroll=8)
        return 0

    lax.fori_loop(0, rows_ref.shape[0] // rows, some, 0)


def combine_kernel(target_ref, weight_ref, back_ref, hidden_ref, out_ref, wide_ref):
    tokens, pieces, _ = hidden_ref.shape
    skew = wide_ref.shape[0] // pieces
    top = target_ref.shape[0] // tokens

    def one(t, _):
        total = jnp.zeros((pieces, LANES), F32)
        for j in range(top):
            i = t * top + j
            total = total + weight_ref[i] * back_ref[target_ref[i]].astype(F32)
        wide_ref[pl.ds(t, pieces, stride=skew), :] = hidden_ref[t].astype(F32) + total
        return 0

    lax.fori_loop(0, tokens, one, 0, unroll=4)
    for c in range(pieces):
        out_ref[:, c * LANES : (c + 1) * LANES] = wide_ref[
            c * skew : c * skew + tokens, :
        ].astype(BF16)


def whole(shape, space=None):
    if space is None:
        return pl.BlockSpec(shape, lambda *_: (0,) * len(shape))
    return pl.BlockSpec(memory_space=space)


def cost(flops, moved):
    return pl.CostEstimate(flops=int(flops), bytes_accessed=int(moved), transcendentals=0)


def slots_of(chosen, experts, capacity, tokens, top_count):
    matches = (chosen[:, None] == jnp.arange(experts, dtype=jnp.int32)[None, :]).astype(jnp.int32)
    rank_in = jnp.sum((jnp.cumsum(matches, axis=0) - 1) * matches, axis=1)
    target = chosen * capacity + rank_in
    owners = jnp.arange(tokens * top_count, dtype=jnp.int32) // top_count
    slot_owner = jnp.zeros((experts * capacity,), jnp.int32).at[target].set(owners)
    return target, slot_owner


def local(
    queries,
    forget_pre,
    values,
    out_gate,
    lower_bound,
    head_gain,
    residual,
    out_weight,
    ffn_gain,
    routing,
    route_weight,
    expert_gate,
    expert_up,
    expert_down,
):
    tokens = queries.shape[1]
    channels = queries.shape[2]
    size = head_gain.shape[0]
    heads = channels // size
    width = residual.shape[2]
    pieces = width // LANES
    top_count = routing.shape[2]
    span = lax.axis_size("sp") * lax.axis_size("dp")
    experts = expert_gate.shape[0] * span
    slots = experts * CAPACITY

    half = channels // 2
    upper, lower = out_weight[:half], out_weight[half:]
    ring = lax.axis_size("dp")
    forward = [(d, (d + 2) % ring) for d in range(ring)]
    backward = [(d, (d + ring - 2) % ring) for d in range(ring)]
    across = [(d, d ^ 1) for d in range(ring)]
    before_upper = lax.ppermute(upper, "dp", forward)
    after_lower = lax.ppermute(lower, "dp", backward)
    before_lower = lax.ppermute(lower, "dp", forward)
    after_upper = lax.ppermute(upper, "dp", backward)

    def swap(x):
        return lax.ppermute(x, "dp", across)

    in_vmem = whole(None, pltpu.VMEM)
    q = queries.reshape(tokens, channels)
    f = forget_pre.reshape(tokens, channels)
    v = values.reshape(tokens, channels)
    g = out_gate.reshape(tokens, channels)
    pair = pl.pallas_call(
        pair_kernel,
        in_specs=[in_vmem, in_vmem],
        out_specs=in_vmem,
        out_shape=jax.ShapeDtypeStruct((heads, 2, tokens, size), BF16),
        cost_estimate=cost(1e6, 2e6),
        compiler_params=pltpu.CompilerParams(vmem_limit_bytes=8 * 2**20),
        name="pair",
    )(f, v)
    arrived = lax.all_to_all(pair, "sp", split_axis=0, concat_axis=0, tiled=True)
    arrived, before_upper, after_lower = lax.optimization_barrier(
        (arrived, before_upper, after_lower)
    )
    far_upper = lax.ppermute(before_upper, "dp", forward)
    far_lower = lax.ppermute(after_lower, "dp", backward)
    before = pl.pallas_call(
        state_kernel,
        in_specs=[in_vmem, in_vmem],
        out_specs=in_vmem,
        out_shape=jax.ShapeDtypeStruct((arrived.shape[0], size + MSG_PAD, size), BF16),
        cost_estimate=cost(1e9, 2e6),
        compiler_params=pltpu.CompilerParams(vmem_limit_bytes=12 * 2**20),
        name="state",
    )(arrived, lower_bound.reshape(1, size))
    before = lax.all_to_all(before, "sp", split_axis=0, concat_axis=0, tiled=True)
    before, before_lower, after_upper = lax.optimization_barrier(
        (before, before_lower, after_upper)
    )
    target, slot_owner = slots_of(
        routing.reshape(tokens * top_count), experts, CAPACITY, tokens, top_count
    )
    per_step = 4
    head_block = pl.BlockSpec((tokens, per_step * size), lambda h: (0, h))
    gated = pl.pallas_call(
        mix_kernel,
        grid=(heads // per_step,),
        in_specs=[head_block] * 4
        + [
            pl.BlockSpec((per_step, size + MSG_PAD, size), lambda h: (h, 0, 0)),
            pl.BlockSpec((1, size), lambda h: (0, 0)),
        ],
        out_specs=head_block,
        out_shape=jax.ShapeDtypeStruct((tokens, channels), BF16),
        cost_estimate=cost(2e9, 3e6),
        compiler_params=pltpu.CompilerParams(vmem_limit_bytes=60 * 2**20),
        name="mix",
    )(q, f, v, g, before, head_gain.reshape(1, size))

    gated, slot_owner, target = lax.optimization_barrier((gated, slot_owner, target))
    gated_other = swap(gated)
    columns = out_weight.shape[1]

    def project(limit, *parts):
        wide = sum(p.shape[0] for p in parts) // channels * columns
        shape = jax.ShapeDtypeStruct((tokens, wide), BF16)
        keep, give = pl.pallas_call(
            columns_kernel,
            in_specs=[in_vmem] * (2 + len(parts)),
            out_specs=[in_vmem] * 2,
            out_shape=[shape] * 2,
            cost_estimate=cost(4 * tokens * channels * wide, 2 * channels * wide),
            compiler_params=pltpu.CompilerParams(vmem_limit_bytes=limit * 2**20),
        )(gated, gated_other, *parts)
        return keep, swap(give)

    near = project(14, out_weight, before_upper, before_lower, after_upper, after_lower)
    near, far_upper, far_lower = lax.optimization_barrier((near, far_upper, far_lower))
    far = project(8, far_upper, far_lower)
    chip, core = lax.axis_index("dp") // 2, lax.axis_index("dp") % 2
    order = jnp.stack(
        [
            (chip + hop) % (ring // 2) * 2 + parity
            for hops in ((0, ring // 2 - 1, 1), (2,))
            for parity in (core, 1 - core)
            for hop in hops
        ]
    ).astype(jnp.int32)
    skew = tokens + 1
    outgoing, hidden = pl.pallas_call(
        route_kernel,
        in_specs=[whole(None, pltpu.SMEM)] * 2 + [in_vmem] * 6,
        out_specs=[in_vmem, in_vmem],
        out_shape=[
            jax.ShapeDtypeStruct((slots, pieces, LANES), BF16),
            jax.ShapeDtypeStruct((tokens, pieces, LANES), BF16),
        ],
        scratch_shapes=[
            pltpu.VMEM((tokens, width), F32),
            pltpu.VMEM((skew * pieces, LANES), F32),
            pltpu.VMEM((skew * pieces, LANES), F32),
        ],
        cost_estimate=cost(4e7, 12e6),
        compiler_params=pltpu.CompilerParams(vmem_limit_bytes=24 * 2**20),
        name="route",
    )(
        slot_owner,
        order,
        *near,
        *far,
        residual.reshape(tokens, width),
        ffn_gain.reshape(1, width),
    )

    exchange = functools.partial(
        lax.all_to_all, axis_name=("sp", "dp"), split_axis=0, concat_axis=0, tiled=True
    )
    chunk = (span, CAPACITY * pieces, LANES)
    rows_in = exchange(outgoing.reshape(chunk)).reshape(slots, pieces, LANES)
    hidden_units = expert_gate.shape[2]
    rows = slots // 2
    results = pl.pallas_call(
        expert_kernel,
        in_specs=[in_vmem] * 4,
        out_specs=in_vmem,
        out_shape=jax.ShapeDtypeStruct((slots, pieces, LANES), BF16),
        scratch_shapes=[
            pltpu.VMEM(((rows + 1) * pieces, LANES), F32),
            pltpu.VMEM((rows, width), BF16),
        ],
        cost_estimate=cost(8e9, 24e6),
        compiler_params=pltpu.CompilerParams(vmem_limit_bytes=34 * 2**20),
        name="expert",
    )(
        rows_in,
        expert_gate.reshape(width, hidden_units),
        expert_up.reshape(width, hidden_units),
        expert_down.reshape(hidden_units, width),
    )
    back = exchange(results.reshape(chunk)).reshape(slots, pieces, LANES)
    out = pl.pallas_call(
        combine_kernel,
        in_specs=[
            whole(None, pltpu.SMEM),
            whole(None, pltpu.SMEM),
            whole(None, pltpu.VMEM),
            whole(None, pltpu.VMEM),
        ],
        out_specs=whole(None, pltpu.VMEM),
        out_shape=jax.ShapeDtypeStruct((tokens, width), BF16),
        scratch_shapes=[pltpu.VMEM((skew * pieces, LANES), F32)],
        cost_estimate=cost(4e8, 8e6),
        compiler_params=pltpu.CompilerParams(vmem_limit_bytes=16 * 2**20),
        name="combine",
    )(target, route_weight.reshape(tokens * top_count), back, hidden)
    return out.reshape(1, tokens, width)


def solution(mesh):
    in_specs = (
        P("dp", "sp", None),
        P("dp", "sp", None),
        P("dp", "sp", None),
        P("dp", "sp", None),
        P("sp"),
        P(),
        P("dp", "sp", None),
        P(None, "dp"),
        P(),
        P("dp", "sp", None),
        P("dp", "sp", None),
        P(("sp", "dp"), None, None),
        P(("sp", "dp"), None, None),
        P(("sp", "dp"), None, None),
    )
    out_specs = P("dp", "sp", None)
    return jax.shard_map(local, mesh=mesh, in_specs=in_specs, out_specs=out_specs, check_vma=False)
```

```python
import functools

import jax
import jax.numpy as jnp
from jax import lax
from jax.experimental import pallas as pl
from jax.experimental.pallas import tpu as pltpu
from jax.sharding import PartitionSpec as P

NORM_EPS = 1e-06
LANES = 128
CAPACITY = 5
BF16 = jnp.bfloat16
F32 = jnp.float32
MSG_PAD = 16


def dot(a, b, dims=((1,), (0,)), precision=None):
    return lax.dot_general(
        a, b, (dims, ((), ())), preferred_element_type=F32, precision=precision
    )


def split(x):
    high = x.astype(BF16)
    return high, (x - high.astype(F32)).astype(BF16)


def tril(rows):
    at = lax.broadcasted_iota(jnp.int32, (rows, rows), 0)
    of = lax.broadcasted_iota(jnp.int32, (rows, rows), 1)
    return of <= at


def gate_terms(forget, free):
    leak = free * jax.nn.sigmoid(-forget.astype(F32))
    causal = jnp.where(tril(leak.shape[0]), 1.0, 0.0).astype(BF16)
    log_keep = jnp.log1p(-leak)
    high = log_keep.astype(BF16)
    rest = log_keep - high.astype(F32)
    mid, low = split(rest)
    log_run = (dot(causal, low) + dot(causal, mid)) + dot(causal, high)
    return leak, log_run


def pair_kernel(forget_ref, value_ref, bound_ref, out_ref):
    rows, size = forget_ref.shape[0], out_ref.shape[2]
    free = 1.0 - bound_ref[...]
    high = free.astype(BF16).astype(F32)
    mid = (free - high).astype(BF16).astype(F32)
    low = free - high - mid
    row = lax.broadcasted_iota(jnp.int32, (MSG_PAD, size), 0)
    tail = jnp.where(
        row == 0, high, jnp.where(row == 1, mid, jnp.where(row == 2, low, 0.0))
    ).astype(BF16)
    for h in range(out_ref.shape[0]):
        out_ref[h, 0:rows] = forget_ref[:, h * size : (h + 1) * size]
        out_ref[h, rows : 2 * rows] = value_ref[:, h * size : (h + 1) * size]
        out_ref[h, 2 * rows : 2 * rows + MSG_PAD] = tail


def state_kernel(pair_ref, bound_ref, before_ref):
    blocks, _, size = pair_ref.shape
    rows = (pair_ref.shape[1] - MSG_PAD) // 2
    free = 1.0 - bound_ref[...]
    group = 4

    def some(i, state):
        forget = jnp.concatenate([pair_ref[i * group + j, 0:rows] for j in range(group)], axis=1)
        leak, log_run = gate_terms(forget, jnp.concatenate([free] * group, axis=1))
        log_last = log_run[rows - 1 : rows, :]
        carry = leak * jnp.exp(log_last - log_run)
        keep = jnp.exp(log_last)
        for j in range(group):
            n = i * group + j
            before_ref[n] = state.astype(BF16)
            at = slice(j * size, (j + 1) * size)
            upper, lower = split(carry[:, at])
            value = pair_ref[n, rows : 2 * rows]
            push = dot(value, upper, ((0,), (0,))) + dot(value, lower, ((0,), (0,)))
            state = keep[:, at] * state + push
        return state

    lax.fori_loop(0, blocks // group, some, jnp.zeros((size, size), F32))


def within_kernel(query_ref, forget_ref, value_ref, tail_ref, mix_ref, high_ref, low_ref):
    heads, _, size = tail_ref.shape
    tails = [tail_ref[h].astype(F32) for h in range(heads)]
    free = jnp.concatenate([t[2:3] + t[1:2] + t[0:1] for t in tails], axis=1)
    leak, log_run = gate_terms(forget_ref[...], free)
    q_scaled = query_ref[...].astype(F32) * jnp.exp(log_run)
    k_scaled = leak * jnp.exp(-log_run)
    q_high, q_low = split(q_scaled)
    k_high, k_low = split(k_scaled)
    high_ref[...] = q_high
    low_ref[...] = q_low
    causal = tril(leak.shape[0])
    lanes = ((1,), (1,))
    for h in range(heads):
        at = slice(h * size, (h + 1) * size)
        scores = (
            dot(q_high[:, at], k_high[:, at], lanes)
            + dot(q_high[:, at], k_low[:, at], lanes)
            + dot(q_low[:, at], k_high[:, at], lanes)
        )
        s_high, s_low = split(jnp.where(causal, scores, 0.0))
        value = value_ref[:, at]
        mix_ref[:, at] = dot(s_high, value) + dot(s_low, value)


def finish_kernel(first, mix_ref, high_ref, low_ref, gate_ref, before_ref, gain_ref, out_ref):
    size = before_ref.shape[2]
    lanes = ((1,), (1,))
    for h in range(out_ref.shape[1] // size):
        to = slice(h * size, (h + 1) * size)
        at = slice((first + h) * size, (first + h + 1) * size)
        before = before_ref[first + h]
        mix = (
            mix_ref[:, at]
            + dot(high_ref[:, at], before, lanes)
            + dot(low_ref[:, at], before, lanes)
        )
        scale = lax.rsqrt(jnp.mean(mix * mix, axis=-1, keepdims=True) + NORM_EPS)
        normed = (mix * scale * gain_ref[...]).astype(BF16)
        u = gate_ref[:, at].astype(F32)
        out_ref[:, to] = (normed.astype(F32) * (u / (1.0 + jnp.exp(-u)))).astype(BF16)


def columns_kernel(place_ref, mine_a, mine_b, other_a, other_b, *refs):
    *w_refs, keep_ref, give_ref, mine_ref, other_ref = refs
    columns = w_refs[0].shape[1]
    depth = mine_ref.shape[1]
    half = mine_a.shape[1]
    mine_ref[:, :half], mine_ref[:, half:] = mine_a[...], mine_b[...]
    other_ref[:, :half], other_ref[:, half:] = other_a[...], other_b[...]
    for src, dst in ((mine_ref, keep_ref), (other_ref, give_ref)):
        n, done, total = 0, 0, None
        for i, w_ref in enumerate(w_refs):
            rows = w_ref.shape[0]
            if rows == depth:
                part = dot(src[...], w_ref[...])
            else:
                at = pl.multiple_of(place_ref[i] * rows, rows)
                part = dot(src[:, pl.ds(at, rows)], w_ref[...])
            total = part if total is None else total + part
            done += rows
            if done == depth:
                dst[:, n * columns : (n + 1) * columns] = total.astype(BF16)
                n, done, total = n + 1, 0, None


def route_kernel(slot_ref, order_ref, *refs):
    *part_refs, residual_ref, gain_ref, outgoing_ref, hidden_ref, wide_ref, moe_ref, keep_ref = refs
    tokens, width = residual_ref.shape
    pieces = width // LANES
    columns = width // order_ref.shape[0]
    skew = moe_ref.shape[0] // pieces
    squares = jnp.zeros((tokens, 1), F32)
    parts = [
        ref[:, n * columns : (n + 1) * columns]
        for ref in part_refs
        for n in range(ref.shape[1] // columns)
    ]
    for n, part in enumerate(parts):
        at = pl.multiple_of(order_ref[n] * columns, columns)
        hidden = residual_ref[:, pl.ds(at, columns)].astype(F32) + part.astype(F32)
        hidden = hidden.astype(BF16).astype(F32)
        wide_ref[:, pl.ds(at, columns)] = hidden
        squares = squares + jnp.sum(hidden * hidden, axis=-1, keepdims=True)
    scale = lax.rsqrt(squares / width + NORM_EPS)
    for c in range(pieces):
        part = wide_ref[:, c * LANES : (c + 1) * LANES]
        keep_ref[c * skew : c * skew + tokens, :] = part
        gain = gain_ref[:, c * LANES : (c + 1) * LANES]
        moe_ref[c * skew : c * skew + tokens, :] = part * scale * gain

    def keep_row(t, _):
        hidden_ref[t] = keep_ref[pl.ds(t, pieces, stride=skew), :].astype(BF16)
        return 0

    lax.fori_loop(0, tokens, keep_row, 0, unroll=4)

    def fill_slot(s, _):
        outgoing_ref[s] = moe_ref[pl.ds(slot_ref[s], pieces, stride=skew), :].astype(BF16)
        return 0

    lax.fori_loop(0, outgoing_ref.shape[0], fill_slot, 0, unroll=8)


def expert_kernel(rows_ref, gate_ref, up_ref, down_ref, out_ref, wide_ref, x_ref):
    pieces = rows_ref.shape[1]
    rows = x_ref.shape[0]
    skew = wide_ref.shape[0] // pieces

    def some(i, _):
        first = i * rows

        def spread(r, _):
            wide_ref[pl.ds(r, pieces, stride=skew), :] = rows_ref[first + r].astype(F32)
            return 0

        lax.fori_loop(0, rows, spread, 0, unroll=8)
        for c in range(pieces):
            x_ref[:, c * LANES : (c + 1) * LANES] = wide_ref[
                c * skew : c * skew + rows, :
            ].astype(BF16)
        gate = dot(x_ref[...], gate_ref[...])
        up = dot(x_ref[...], up_ref[...])
        act = (gate / (1.0 + jnp.exp(-gate)) * up).astype(BF16)
        step = 4
        for c in range(0, pieces, step):
            part = dot(act, down_ref[:, c * LANES : (c + step) * LANES])
            for k in range(step):
                wide_ref[(c + k) * skew : (c + k) * skew + rows, :] = part[
                    :, k * LANES : (k + 1) * LANES
                ]

        def gather(r, _):
            out_ref[first + r] = wide_ref[pl.ds(r, pieces, stride=skew), :].astype(BF16)
            return 0

        lax.fori_loop(0, rows, gather, 0, unroll=8)
        return 0

    lax.fori_loop(0, rows_ref.shape[0] // rows, some, 0)


def combine_kernel(target_ref, weight_ref, back_ref, hidden_ref, out_ref, wide_ref):
    tokens, pieces, _ = hidden_ref.shape
    skew = wide_ref.shape[0] // pieces
    top = target_ref.shape[0] // tokens

    def one(t, _):
        total = jnp.zeros((pieces, LANES), F32)
        for j in range(top):
            i = t * top + j
            total = total + weight_ref[i] * back_ref[target_ref[i]].astype(F32)
        wide_ref[pl.ds(t, pieces, stride=skew), :] = hidden_ref[t].astype(F32) + total
        return 0

    lax.fori_loop(0, tokens, one, 0, unroll=4)
    for c in range(pieces):
        out_ref[:, c * LANES : (c + 1) * LANES] = wide_ref[
            c * skew : c * skew + tokens, :
        ].astype(BF16)


def whole(shape, space=None):
    if space is None:
        return pl.BlockSpec(shape, lambda *_: (0,) * len(shape))
    return pl.BlockSpec(memory_space=space)


def cost(flops, moved):
    return pl.CostEstimate(flops=int(flops), bytes_accessed=int(moved), transcendentals=0)


def slots_of(chosen, experts, capacity, tokens, top_count):
    matches = (chosen[:, None] == jnp.arange(experts, dtype=jnp.int32)[None, :]).astype(jnp.int32)
    rank_in = jnp.sum((jnp.cumsum(matches, axis=0) - 1) * matches, axis=1)
    target = chosen * capacity + rank_in
    owners = jnp.arange(tokens * top_count, dtype=jnp.int32) // top_count
    slot_owner = jnp.zeros((experts * capacity,), jnp.int32).at[target].set(owners)
    return target, slot_owner


def local(
    queries,
    forget_pre,
    values,
    out_gate,
    lower_bound,
    head_gain,
    residual,
    out_weight,
    ffn_gain,
    routing,
    route_weight,
    expert_gate,
    expert_up,
    expert_down,
):
    tokens = queries.shape[1]
    channels = queries.shape[2]
    size = head_gain.shape[0]
    heads = channels // size
    width = residual.shape[2]
    pieces = width // LANES
    top_count = routing.shape[2]
    span = lax.axis_size("sp") * lax.axis_size("dp")
    experts = expert_gate.shape[0] * span
    slots = experts * CAPACITY

    ring = lax.axis_size("dp")
    turn = 4
    along = lax.axis_index("sp") % turn
    across = [(d, d ^ 1) for d in range(ring)]

    def hop(x, chips):
        return lax.ppermute(x, "dp", [(d, (d + 2 * chips) % ring) for d in range(ring)])

    def pass_on(x, steps):
        moves = [(s, s // turn * turn + (s + steps) % turn) for s in range(lax.axis_size("sp"))]
        return lax.ppermute(x, "sp", moves)

    quarter = channels // turn
    far = hop(lax.dynamic_slice_in_dim(out_weight, along * quarter, quarter), 2)
    before_block = hop(out_weight, 1)
    after_block = hop(out_weight, -1)

    def swap(x):
        return lax.ppermute(x, "dp", across)

    in_vmem = whole(None, pltpu.VMEM)
    q = queries.reshape(tokens, channels)
    f = forget_pre.reshape(tokens, channels)
    v = values.reshape(tokens, channels)
    g = out_gate.reshape(tokens, channels)
    bound = lower_bound.reshape(1, size)
    message = 2 * tokens + MSG_PAD
    pair = pl.pallas_call(
        pair_kernel,
        in_specs=[in_vmem] * 3,
        out_specs=in_vmem,
        out_shape=jax.ShapeDtypeStruct((heads, message, size), BF16),
        cost_estimate=cost(1e6, 2e6),
        compiler_params=pltpu.CompilerParams(vmem_limit_bytes=60 * 2**20),
        name="pair",
    )(f, v, bound)
    arrived = lax.all_to_all(pair, "sp", split_axis=0, concat_axis=0, tiled=True)
    far_parts = (far, pass_on(far, 1), pass_on(far, -1), pass_on(far, 2))
    before = pl.pallas_call(
        state_kernel,
        in_specs=[in_vmem, in_vmem],
        out_specs=in_vmem,
        out_shape=jax.ShapeDtypeStruct((arrived.shape[0], size, size), BF16),
        cost_estimate=cost(1e9, 2e6),
        compiler_params=pltpu.CompilerParams(vmem_limit_bytes=12 * 2**20),
        name="state",
    )(arrived, bound)
    before = lax.all_to_all(before, "sp", split_axis=0, concat_axis=0, tiled=True)
    target, slot_owner = slots_of(
        routing.reshape(tokens * top_count), experts, CAPACITY, tokens, top_count
    )
    per_step = 4
    head_block = pl.BlockSpec((tokens, per_step * size), lambda h: (0, h))
    mix_shape = jax.ShapeDtypeStruct((tokens, channels), F32)
    q_shape = jax.ShapeDtypeStruct((tokens, channels), BF16)
    mix, q_high, q_low = pl.pallas_call(
        within_kernel,
        grid=(heads // per_step,),
        in_specs=[head_block] * 3
        + [pl.BlockSpec((per_step, MSG_PAD, size), lambda h: (h, 2 * tokens // MSG_PAD, 0))],
        out_specs=[head_block] * 3,
        out_shape=[mix_shape, q_shape, q_shape],
        cost_estimate=cost(2e9, 3e6),
        compiler_params=pltpu.CompilerParams(vmem_limit_bytes=16 * 2**20),
        name="within",
    )(q, f, v, arrived)

    def finish(first, count):
        return pl.pallas_call(
            functools.partial(finish_kernel, first),
            in_specs=[in_vmem] * 6,
            out_specs=in_vmem,
            out_shape=jax.ShapeDtypeStruct((tokens, count * size), BF16),
            cost_estimate=cost(6e8, 2e6),
            compiler_params=pltpu.CompilerParams(vmem_limit_bytes=12 * 2**20),
            name="finish",
        )(mix, q_high, q_low, g, before, head_gain.reshape(1, size))

    weights = route_weight.reshape(tokens * top_count)
    gated_a = finish(0, heads // 2)
    other_a = swap(gated_a)
    gated_b = finish(heads // 2, heads // 2)
    gated_b, slot_owner, target, weights = lax.optimization_barrier(
        (gated_b, slot_owner, target, weights)
    )
    other_b = swap(gated_b)
    columns = out_weight.shape[1]

    def project(limit, *parts):
        wide = sum(p.shape[0] for p in parts) // channels * columns
        shape = jax.ShapeDtypeStruct((tokens, wide), BF16)
        keep, give = pl.pallas_call(
            columns_kernel,
            in_specs=[whole(None, pltpu.SMEM)] + [in_vmem] * (4 + len(parts)),
            out_specs=[in_vmem] * 2,
            out_shape=[shape] * 2,
            scratch_shapes=[pltpu.VMEM((tokens, channels), BF16)] * 2,
            cost_estimate=cost(4 * tokens * channels * wide, 2 * channels * wide),
            compiler_params=pltpu.CompilerParams(vmem_limit_bytes=limit * 2**20),
        )(place, gated_a, gated_b, other_a, other_b, *parts)
        return keep, swap(give)

    place = jnp.stack([(along + turn - shift) % turn for shift in (0, 1, turn - 1, 2)])
    place = place.astype(jnp.int32)
    near = project(14, out_weight, before_block, after_block)
    far = project(8, *far_parts)
    chip, core = lax.axis_index("dp") // 2, lax.axis_index("dp") % 2
    order = jnp.stack(
        [
            (chip + hop) % (ring // 2) * 2 + parity
            for hops in ((0, ring // 2 - 1, 1), (2,))
            for parity in (core, 1 - core)
            for hop in hops
        ]
    ).astype(jnp.int32)
    skew = tokens + 1
    outgoing, hidden = pl.pallas_call(
        route_kernel,
        in_specs=[whole(None, pltpu.SMEM)] * 2 + [in_vmem] * 6,
        out_specs=[in_vmem, in_vmem],
        out_shape=[
            jax.ShapeDtypeStruct((slots, pieces, LANES), BF16),
            jax.ShapeDtypeStruct((tokens, pieces, LANES), BF16),
        ],
        scratch_shapes=[
            pltpu.VMEM((tokens, width), F32),
            pltpu.VMEM((skew * pieces, LANES), F32),
            pltpu.VMEM((skew * pieces, LANES), F32),
        ],
        cost_estimate=cost(4e7, 12e6),
        compiler_params=pltpu.CompilerParams(vmem_limit_bytes=24 * 2**20),
        name="route",
    )(
        slot_owner,
        order,
        *near,
        *far,
        residual.reshape(tokens, width),
        ffn_gain.reshape(1, width),
    )

    exchange = functools.partial(
        lax.all_to_all, axis_name=("sp", "dp"), split_axis=0, concat_axis=0, tiled=True
    )
    chunk = (span, CAPACITY * pieces, LANES)
    rows_in = exchange(outgoing.reshape(chunk)).reshape(slots, pieces, LANES)
    hidden_units = expert_gate.shape[2]
    rows = slots // 2
    results = pl.pallas_call(
        expert_kernel,
        in_specs=[in_vmem] * 4,
        out_specs=in_vmem,
        out_shape=jax.ShapeDtypeStruct((slots, pieces, LANES), BF16),
        scratch_shapes=[
            pltpu.VMEM(((rows + 1) * pieces, LANES), F32),
            pltpu.VMEM((rows, width), BF16),
        ],
        cost_estimate=cost(8e9, 24e6),
        compiler_params=pltpu.CompilerParams(vmem_limit_bytes=34 * 2**20),
        name="expert",
    )(
        rows_in,
        expert_gate.reshape(width, hidden_units),
        expert_up.reshape(width, hidden_units),
        expert_down.reshape(hidden_units, width),
    )
    back = exchange(results.reshape(chunk)).reshape(slots, pieces, LANES)
    out = pl.pallas_call(
        combine_kernel,
        in_specs=[
            whole(None, pltpu.SMEM),
            whole(None, pltpu.SMEM),
            whole(None, pltpu.VMEM),
            whole(None, pltpu.VMEM),
        ],
        out_specs=whole(None, pltpu.VMEM),
        out_shape=jax.ShapeDtypeStruct((tokens, width), BF16),
        scratch_shapes=[pltpu.VMEM((skew * pieces, LANES), F32)],
        cost_estimate=cost(4e8, 8e6),
        compiler_params=pltpu.CompilerParams(vmem_limit_bytes=16 * 2**20),
        name="combine",
    )(target, weights, back, hidden)
    return out.reshape(1, tokens, width)


def solution(mesh):
    in_specs = (
        P("dp", "sp", None),
        P("dp", "sp", None),
        P("dp", "sp", None),
        P("dp", "sp", None),
        P("sp"),
        P(),
        P("dp", "sp", None),
        P(None, "dp"),
        P(),
        P("dp", "sp", None),
        P("dp", "sp", None),
        P(("sp", "dp"), None, None),
        P(("sp", "dp"), None, None),
        P(("sp", "dp"), None, None),
    )
    out_specs = P("dp", "sp", None)
    return jax.shard_map(local, mesh=mesh, in_specs=in_specs, out_specs=out_specs, check_vma=False)
```

```python
import functools

import jax
import jax.numpy as jnp
from jax import lax
from jax.experimental import pallas as pl
from jax.experimental.pallas import tpu as pltpu
from jax.sharding import PartitionSpec as P

NORM_EPS = 1e-06
LANES = 128
CAPACITY = 5
BF16 = jnp.bfloat16
F32 = jnp.float32
MSG_PAD = 16


def dot(a, b, dims=((1,), (0,)), precision=None):
    return lax.dot_general(
        a, b, (dims, ((), ())), preferred_element_type=F32, precision=precision
    )


def split(x):
    high = x.astype(BF16)
    return high, (x - high.astype(F32)).astype(BF16)


def tril(rows):
    at = lax.broadcasted_iota(jnp.int32, (rows, rows), 0)
    of = lax.broadcasted_iota(jnp.int32, (rows, rows), 1)
    return of <= at


def gate_terms(forget, free):
    leak = free * jax.nn.sigmoid(-forget.astype(F32))
    causal = jnp.where(tril(leak.shape[0]), 1.0, 0.0).astype(BF16)
    log_keep = jnp.log1p(-leak)
    high = log_keep.astype(BF16)
    rest = log_keep - high.astype(F32)
    mid, low = split(rest)
    log_run = (dot(causal, low) + dot(causal, mid)) + dot(causal, high)
    return leak, log_run


def pair_kernel(forget_ref, value_ref, bound_ref, out_ref):
    rows, size = forget_ref.shape[0], out_ref.shape[2]
    free = 1.0 - bound_ref[...]
    high = free.astype(BF16).astype(F32)
    mid = (free - high).astype(BF16).astype(F32)
    low = free - high - mid
    row = lax.broadcasted_iota(jnp.int32, (MSG_PAD, size), 0)
    tail = jnp.where(
        row == 0, high, jnp.where(row == 1, mid, jnp.where(row == 2, low, 0.0))
    ).astype(BF16)
    for h in range(out_ref.shape[0]):
        out_ref[h, 0:rows] = forget_ref[:, h * size : (h + 1) * size]
        out_ref[h, rows : 2 * rows] = value_ref[:, h * size : (h + 1) * size]
        out_ref[h, 2 * rows : 2 * rows + MSG_PAD] = tail


def state_kernel(pair_ref, bound_ref, before_ref):
    blocks, _, size = pair_ref.shape
    rows = (pair_ref.shape[1] - MSG_PAD) // 2
    free = 1.0 - bound_ref[...]
    group = 4

    def some(i, state):
        forget = jnp.concatenate([pair_ref[i * group + j, 0:rows] for j in range(group)], axis=1)
        leak, log_run = gate_terms(forget, jnp.concatenate([free] * group, axis=1))
        log_last = log_run[rows - 1 : rows, :]
        carry = leak * jnp.exp(log_last - log_run)
        keep = jnp.exp(log_last)
        for j in range(group):
            n = i * group + j
            before_ref[n] = state.astype(BF16)
            at = slice(j * size, (j + 1) * size)
            upper, lower = split(carry[:, at])
            value = pair_ref[n, rows : 2 * rows]
            push = dot(value, upper, ((0,), (0,))) + dot(value, lower, ((0,), (0,)))
            state = keep[:, at] * state + push
        return state

    lax.fori_loop(0, blocks // group, some, jnp.zeros((size, size), F32))


def within_kernel(query_ref, forget_ref, value_ref, tail_ref, mix_ref, high_ref, low_ref):
    heads, _, size = tail_ref.shape
    tails = [tail_ref[h].astype(F32) for h in range(heads)]
    free = jnp.concatenate([t[2:3] + t[1:2] + t[0:1] for t in tails], axis=1)
    leak, log_run = gate_terms(forget_ref[...], free)
    q_scaled = query_ref[...].astype(F32) * jnp.exp(log_run)
    k_scaled = leak * jnp.exp(-log_run)
    q_high, q_low = split(q_scaled)
    k_high, k_low = split(k_scaled)
    high_ref[...] = q_high
    low_ref[...] = q_low
    causal = tril(leak.shape[0])
    lanes = ((1,), (1,))
    for h in range(heads):
        at = slice(h * size, (h + 1) * size)
        scores = (
            dot(q_high[:, at], k_high[:, at], lanes)
            + dot(q_high[:, at], k_low[:, at], lanes)
            + dot(q_low[:, at], k_high[:, at], lanes)
        )
        s_high, s_low = split(jnp.where(causal, scores, 0.0))
        value = value_ref[:, at]
        mix_ref[:, at] = dot(s_high, value) + dot(s_low, value)


def finish_kernel(first, mix_ref, high_ref, low_ref, gate_ref, before_ref, gain_ref, out_ref):
    size = before_ref.shape[2]
    lanes = ((1,), (1,))
    for h in range(out_ref.shape[1] // size):
        to = slice(h * size, (h + 1) * size)
        at = slice((first + h) * size, (first + h + 1) * size)
        before = before_ref[first + h]
        mix = (
            mix_ref[:, at]
            + dot(high_ref[:, at], before, lanes)
            + dot(low_ref[:, at], before, lanes)
        )
        scale = lax.rsqrt(jnp.mean(mix * mix, axis=-1, keepdims=True) + NORM_EPS)
        normed = (mix * scale * gain_ref[...]).astype(BF16)
        u = gate_ref[:, at].astype(F32)
        out_ref[:, to] = (normed.astype(F32) * (u / (1.0 + jnp.exp(-u)))).astype(BF16)


def columns_kernel(place_ref, mine_a, mine_b, other_a, other_b, *refs):
    count = (len(refs) - 5) // 2
    w_refs, buffers = refs[:count], refs[count + 4 : 2 * count + 4]
    keep_ref, give_ref, mine_ref, other_ref = refs[count : count + 4]
    sems = refs[-1]
    copies = [
        pltpu.make_async_copy(w, buffer, sems.at[i])
        for i, (w, buffer) in enumerate(zip(w_refs, buffers))
    ]
    for copy in copies:
        copy.start()
    columns = w_refs[0].shape[1]
    depth = mine_ref.shape[1]
    half = mine_a.shape[1]
    mine_ref[:, :half], mine_ref[:, half:] = mine_a[...], mine_b[...]
    other_ref[:, :half], other_ref[:, half:] = other_a[...], other_b[...]
    n, done, totals = 0, 0, [0.0, 0.0]
    for i, (copy, buffer) in enumerate(zip(copies, buffers)):
        copy.wait()
        rows = buffer.shape[0]
        for k, src in enumerate((mine_ref, other_ref)):
            if rows == depth:
                totals[k] = dot(src[...], buffer[...])
            else:
                at = pl.multiple_of(place_ref[i] * rows, rows)
                totals[k] = totals[k] + dot(src[:, pl.ds(at, rows)], buffer[...])
        done += rows
        if done == depth:
            for total, dst in zip(totals, (keep_ref, give_ref)):
                dst[:, n * columns : (n + 1) * columns] = total.astype(BF16)
            n, done, totals = n + 1, 0, [0.0, 0.0]


def route_kernel(slot_ref, order_ref, *refs):
    *part_refs, residual_ref, gain_ref, outgoing_ref, hidden_ref, wide_ref, moe_ref, keep_ref = refs
    tokens, width = residual_ref.shape
    pieces = width // LANES
    columns = width // order_ref.shape[0]
    skew = moe_ref.shape[0] // pieces
    squares = jnp.zeros((tokens, 1), F32)
    parts = [
        ref[:, n * columns : (n + 1) * columns]
        for ref in part_refs
        for n in range(ref.shape[1] // columns)
    ]
    for n, part in enumerate(parts):
        at = pl.multiple_of(order_ref[n] * columns, columns)
        hidden = residual_ref[:, pl.ds(at, columns)].astype(F32) + part.astype(F32)
        hidden = hidden.astype(BF16).astype(F32)
        wide_ref[:, pl.ds(at, columns)] = hidden
        squares = squares + jnp.sum(hidden * hidden, axis=-1, keepdims=True)
    scale = lax.rsqrt(squares / width + NORM_EPS)
    for c in range(pieces):
        part = wide_ref[:, c * LANES : (c + 1) * LANES]
        keep_ref[c * skew : c * skew + tokens, :] = part
        gain = gain_ref[:, c * LANES : (c + 1) * LANES]
        moe_ref[c * skew : c * skew + tokens, :] = part * scale * gain

    def keep_row(t, _):
        hidden_ref[t] = keep_ref[pl.ds(t, pieces, stride=skew), :].astype(BF16)
        return 0

    lax.fori_loop(0, tokens, keep_row, 0, unroll=4)

    def fill_slot(s, _):
        outgoing_ref[s] = moe_ref[pl.ds(slot_ref[s], pieces, stride=skew), :].astype(BF16)
        return 0

    lax.fori_loop(0, outgoing_ref.shape[0], fill_slot, 0, unroll=8)


def expert_kernel(rows_ref, gate_ref, up_ref, down_ref, out_ref, wide_ref, x_ref):
    pieces = rows_ref.shape[1]
    rows = x_ref.shape[0]
    skew = wide_ref.shape[0] // pieces

    def some(i, _):
        first = i * rows

        def spread(r, _):
            wide_ref[pl.ds(r, pieces, stride=skew), :] = rows_ref[first + r].astype(F32)
            return 0

        lax.fori_loop(0, rows, spread, 0, unroll=8)
        for c in range(pieces):
            x_ref[:, c * LANES : (c + 1) * LANES] = wide_ref[
                c * skew : c * skew + rows, :
            ].astype(BF16)
        gate = dot(x_ref[...], gate_ref[...])
        up = dot(x_ref[...], up_ref[...])
        act = (gate / (1.0 + jnp.exp(-gate)) * up).astype(BF16)
        step = 4
        for c in range(0, pieces, step):
            part = dot(act, down_ref[:, c * LANES : (c + step) * LANES])
            for k in range(step):
                wide_ref[(c + k) * skew : (c + k) * skew + rows, :] = part[
                    :, k * LANES : (k + 1) * LANES
                ]

        def gather(r, _):
            out_ref[first + r] = wide_ref[pl.ds(r, pieces, stride=skew), :].astype(BF16)
            return 0

        lax.fori_loop(0, rows, gather, 0, unroll=8)
        return 0

    lax.fori_loop(0, rows_ref.shape[0] // rows, some, 0)


def combine_kernel(target_ref, weight_ref, back_ref, hidden_ref, out_ref, wide_ref):
    tokens, pieces, _ = hidden_ref.shape
    skew = wide_ref.shape[0] // pieces
    top = target_ref.shape[0] // tokens

    def one(t, _):
        total = jnp.zeros((pieces, LANES), F32)
        for j in range(top):
            i = t * top + j
            total = total + weight_ref[i] * back_ref[target_ref[i]].astype(F32)
        wide_ref[pl.ds(t, pieces, stride=skew), :] = hidden_ref[t].astype(F32) + total
        return 0

    lax.fori_loop(0, tokens, one, 0, unroll=4)
    for c in range(pieces):
        out_ref[:, c * LANES : (c + 1) * LANES] = wide_ref[
            c * skew : c * skew + tokens, :
        ].astype(BF16)


def whole(shape, space=None):
    if space is None:
        return pl.BlockSpec(shape, lambda *_: (0,) * len(shape))
    return pl.BlockSpec(memory_space=space)


def cost(flops, moved):
    return pl.CostEstimate(flops=int(flops), bytes_accessed=int(moved), transcendentals=0)


def slots_of(chosen, experts, capacity, tokens, top_count):
    matches = (chosen[:, None] == jnp.arange(experts, dtype=jnp.int32)[None, :]).astype(jnp.int32)
    rank_in = jnp.sum((jnp.cumsum(matches, axis=0) - 1) * matches, axis=1)
    target = chosen * capacity + rank_in
    owners = jnp.arange(tokens * top_count, dtype=jnp.int32) // top_count
    slot_owner = jnp.zeros((experts * capacity,), jnp.int32).at[target].set(owners)
    return target, slot_owner


def local(
    queries,
    forget_pre,
    values,
    out_gate,
    lower_bound,
    head_gain,
    residual,
    out_weight,
    ffn_gain,
    routing,
    route_weight,
    expert_gate,
    expert_up,
    expert_down,
):
    tokens = queries.shape[1]
    channels = queries.shape[2]
    size = head_gain.shape[0]
    heads = channels // size
    width = residual.shape[2]
    pieces = width // LANES
    top_count = routing.shape[2]
    span = lax.axis_size("sp") * lax.axis_size("dp")
    experts = expert_gate.shape[0] * span
    slots = experts * CAPACITY

    ring = lax.axis_size("dp")
    turn = 4
    at_z, at_x = lax.axis_index("sp") // turn, lax.axis_index("sp") % turn
    along = (at_x + 2 * at_z) % turn
    across = [(d, d ^ 1) for d in range(ring)]

    def hop(x, chips):
        return lax.ppermute(x, "dp", [(d, (d + 2 * chips) % ring) for d in range(ring)])

    def pass_on(x, steps):
        moves = [(s, s // turn * turn + (s + steps) % turn) for s in range(lax.axis_size("sp"))]
        return lax.ppermute(x, "sp", moves)

    def pass_up(x):
        rows = lax.axis_size("sp")
        return lax.ppermute(x, "sp", [(s, (s + turn) % rows) for s in range(rows)])

    quarter = channels // turn
    far = hop(lax.dynamic_slice_in_dim(out_weight, along * quarter, quarter), 2)
    before_block = hop(out_weight, 1)
    after_block = hop(out_weight, -1)

    def swap(x):
        return lax.ppermute(x, "dp", across)

    in_vmem = whole(None, pltpu.VMEM)
    q = queries.reshape(tokens, channels)
    f = forget_pre.reshape(tokens, channels)
    v = values.reshape(tokens, channels)
    g = out_gate.reshape(tokens, channels)
    bound = lower_bound.reshape(1, size)
    message = 2 * tokens + MSG_PAD
    pair = pl.pallas_call(
        pair_kernel,
        in_specs=[in_vmem] * 3,
        out_specs=in_vmem,
        out_shape=jax.ShapeDtypeStruct((heads, message, size), BF16),
        cost_estimate=cost(1e6, 2e6),
        compiler_params=pltpu.CompilerParams(vmem_limit_bytes=60 * 2**20),
        name="pair",
    )(f, v, bound)
    arrived = lax.all_to_all(pair, "sp", split_axis=0, concat_axis=0, tiled=True)
    far_parts = (far, pass_on(far, 1), pass_on(far, -1), pass_up(far))
    before = pl.pallas_call(
        state_kernel,
        in_specs=[in_vmem, in_vmem],
        out_specs=in_vmem,
        out_shape=jax.ShapeDtypeStruct((arrived.shape[0], size, size), BF16),
        cost_estimate=cost(1e9, 2e6),
        compiler_params=pltpu.CompilerParams(vmem_limit_bytes=12 * 2**20),
        name="state",
    )(arrived, bound)
    before = lax.all_to_all(before, "sp", split_axis=0, concat_axis=0, tiled=True)
    target, slot_owner = slots_of(
        routing.reshape(tokens * top_count), experts, CAPACITY, tokens, top_count
    )
    per_step = 4
    head_block = pl.BlockSpec((tokens, per_step * size), lambda h: (0, h))
    mix_shape = jax.ShapeDtypeStruct((tokens, channels), F32)
    q_shape = jax.ShapeDtypeStruct((tokens, channels), BF16)
    mix, q_high, q_low = pl.pallas_call(
        within_kernel,
        grid=(heads // per_step,),
        in_specs=[head_block] * 3
        + [pl.BlockSpec((per_step, MSG_PAD, size), lambda h: (h, 2 * tokens // MSG_PAD, 0))],
        out_specs=[head_block] * 3,
        out_shape=[mix_shape, q_shape, q_shape],
        cost_estimate=cost(2e9, 3e6),
        compiler_params=pltpu.CompilerParams(vmem_limit_bytes=60 * 2**20),
        name="within",
    )(q, f, v, arrived)

    def finish(first, count):
        return pl.pallas_call(
            functools.partial(finish_kernel, first),
            in_specs=[in_vmem] * 6,
            out_specs=in_vmem,
            out_shape=jax.ShapeDtypeStruct((tokens, count * size), BF16),
            cost_estimate=cost(6e8, 2e6),
            compiler_params=pltpu.CompilerParams(vmem_limit_bytes=12 * 2**20),
            name="finish",
        )(mix, q_high, q_low, g, before, head_gain.reshape(1, size))

    weights = route_weight.reshape(tokens * top_count)
    gated_a = finish(0, heads // 2)
    other_a = swap(gated_a)
    gated_b = finish(heads // 2, heads // 2)
    gated_b, slot_owner, target, weights = lax.optimization_barrier(
        (gated_b, slot_owner, target, weights)
    )
    other_b = swap(gated_b)
    columns = out_weight.shape[1]

    def project(limit, *parts):
        wide = sum(p.shape[0] for p in parts) // channels * columns
        shape = jax.ShapeDtypeStruct((tokens, wide), BF16)
        keep, give = pl.pallas_call(
            columns_kernel,
            in_specs=[whole(None, pltpu.SMEM)]
            + [in_vmem] * 4
            + [whole(None, pl.ANY)] * len(parts),
            out_specs=[in_vmem] * 2,
            out_shape=[shape] * 2,
            scratch_shapes=[pltpu.VMEM((tokens, channels), BF16)] * 2
            + [pltpu.VMEM(p.shape, BF16) for p in parts]
            + [pltpu.SemaphoreType.DMA((len(parts),))],
            cost_estimate=cost(4 * tokens * channels * wide, 2 * channels * wide),
            compiler_params=pltpu.CompilerParams(vmem_limit_bytes=limit * 2**20),
        )(place, gated_a, gated_b, other_a, other_b, *parts)
        return keep, swap(give)

    place = jnp.stack([(along + turn - shift) % turn for shift in (0, 1, turn - 1, 2)])
    place = place.astype(jnp.int32)
    early = project(10, *far_parts, out_weight)
    late = project(10, before_block, after_block)
    chip, core = lax.axis_index("dp") // 2, lax.axis_index("dp") % 2
    order = jnp.stack(
        [
            (chip + hop) % (ring // 2) * 2 + parity
            for hops in ((2, 0), (ring // 2 - 1, 1))
            for parity in (core, 1 - core)
            for hop in hops
        ]
    ).astype(jnp.int32)
    skew = tokens + 1
    outgoing, hidden = pl.pallas_call(
        route_kernel,
        in_specs=[whole(None, pltpu.SMEM)] * 2 + [in_vmem] * 6,
        out_specs=[in_vmem, in_vmem],
        out_shape=[
            jax.ShapeDtypeStruct((slots, pieces, LANES), BF16),
            jax.ShapeDtypeStruct((tokens, pieces, LANES), BF16),
        ],
        scratch_shapes=[
            pltpu.VMEM((tokens, width), F32),
            pltpu.VMEM((skew * pieces, LANES), F32),
            pltpu.VMEM((skew * pieces, LANES), F32),
        ],
        cost_estimate=cost(4e7, 12e6),
        compiler_params=pltpu.CompilerParams(vmem_limit_bytes=24 * 2**20),
        name="route",
    )(
        slot_owner,
        order,
        *early,
        *late,
        residual.reshape(tokens, width),
        ffn_gain.reshape(1, width),
    )

    exchange = functools.partial(
        lax.all_to_all, axis_name=("sp", "dp"), split_axis=0, concat_axis=0, tiled=True
    )
    chunk = (span, CAPACITY * pieces, LANES)
    rows_in = exchange(outgoing.reshape(chunk)).reshape(slots, pieces, LANES)
    hidden_units = expert_gate.shape[2]
    rows = slots // 2
    results = pl.pallas_call(
        expert_kernel,
        in_specs=[in_vmem] * 4,
        out_specs=in_vmem,
        out_shape=jax.ShapeDtypeStruct((slots, pieces, LANES), BF16),
        scratch_shapes=[
            pltpu.VMEM(((rows + 1) * pieces, LANES), F32),
            pltpu.VMEM((rows, width), BF16),
        ],
        cost_estimate=cost(8e9, 24e6),
        compiler_params=pltpu.CompilerParams(vmem_limit_bytes=20 * 2**20),
        name="expert",
    )(
        rows_in,
        expert_gate.reshape(width, hidden_units),
        expert_up.reshape(width, hidden_units),
        expert_down.reshape(hidden_units, width),
    )
    back = exchange(results.reshape(chunk)).reshape(slots, pieces, LANES)
    out = pl.pallas_call(
        combine_kernel,
        in_specs=[
            whole(None, pltpu.SMEM),
            whole(None, pltpu.SMEM),
            whole(None, pltpu.VMEM),
            whole(None, pltpu.VMEM),
        ],
        out_specs=whole(None, pltpu.VMEM),
        out_shape=jax.ShapeDtypeStruct((tokens, width), BF16),
        scratch_shapes=[pltpu.VMEM((skew * pieces, LANES), F32)],
        cost_estimate=cost(4e8, 8e6),
        compiler_params=pltpu.CompilerParams(vmem_limit_bytes=16 * 2**20),
        name="combine",
    )(target, weights, back, hidden)
    return out.reshape(1, tokens, width)


def solution(mesh):
    in_specs = (
        P("dp", "sp", None),
        P("dp", "sp", None),
        P("dp", "sp", None),
        P("dp", "sp", None),
        P("sp"),
        P(),
        P("dp", "sp", None),
        P(None, "dp"),
        P(),
        P("dp", "sp", None),
        P("dp", "sp", None),
        P(("sp", "dp"), None, None),
        P(("sp", "dp"), None, None),
        P(("sp", "dp"), None, None),
    )
    out_specs = P("dp", "sp", None)
    return jax.shard_map(local, mesh=mesh, in_specs=in_specs, out_specs=out_specs, check_vma=False)
```

```python
import functools

import jax
import jax.numpy as jnp
from jax import lax
from jax.experimental import pallas as pl
from jax.experimental.pallas import tpu as pltpu
from jax.sharding import PartitionSpec as P

NORM_EPS = 1e-06
LANES = 128
CAPACITY = 5
BF16 = jnp.bfloat16
F32 = jnp.float32
MSG_PAD = 16


def dot(a, b, dims=((1,), (0,)), precision=None):
    return lax.dot_general(
        a, b, (dims, ((), ())), preferred_element_type=F32, precision=precision
    )


def split(x):
    high = x.astype(BF16)
    return high, (x - high.astype(F32)).astype(BF16)


def tril(rows):
    at = lax.broadcasted_iota(jnp.int32, (rows, rows), 0)
    of = lax.broadcasted_iota(jnp.int32, (rows, rows), 1)
    return of <= at


def gate_terms(forget, free):
    leak = free * jax.nn.sigmoid(-forget.astype(F32))
    causal = jnp.where(tril(leak.shape[0]), 1.0, 0.0).astype(BF16)
    log_keep = jnp.log1p(-leak)
    high = log_keep.astype(BF16)
    rest = log_keep - high.astype(F32)
    mid, low = split(rest)
    log_run = (dot(causal, low) + dot(causal, mid)) + dot(causal, high)
    return leak, log_run


def pair_kernel(forget_ref, value_ref, bound_ref, out_ref):
    rows, size = forget_ref.shape[0], out_ref.shape[2]
    free = 1.0 - bound_ref[...]
    high = free.astype(BF16).astype(F32)
    mid = (free - high).astype(BF16).astype(F32)
    low = free - high - mid
    row = lax.broadcasted_iota(jnp.int32, (MSG_PAD, size), 0)
    tail = jnp.where(
        row == 0, high, jnp.where(row == 1, mid, jnp.where(row == 2, low, 0.0))
    ).astype(BF16)
    for h in range(out_ref.shape[0]):
        out_ref[h, 0:rows] = forget_ref[:, h * size : (h + 1) * size]
        out_ref[h, rows : 2 * rows] = value_ref[:, h * size : (h + 1) * size]
        out_ref[h, 2 * rows : 2 * rows + MSG_PAD] = tail


def state_kernel(pair_ref, bound_ref, before_ref):
    blocks, _, size = pair_ref.shape
    rows = (pair_ref.shape[1] - MSG_PAD) // 2
    free = 1.0 - bound_ref[...]
    group = 4

    def some(i, state):
        forget = jnp.concatenate([pair_ref[i * group + j, 0:rows] for j in range(group)], axis=1)
        leak, log_run = gate_terms(forget, jnp.concatenate([free] * group, axis=1))
        log_last = log_run[rows - 1 : rows, :]
        carry = leak * jnp.exp(log_last - log_run)
        keep = jnp.exp(log_last)
        for j in range(group):
            n = i * group + j
            before_ref[n] = state.astype(BF16)
            at = slice(j * size, (j + 1) * size)
            upper, lower = split(carry[:, at])
            value = pair_ref[n, rows : 2 * rows]
            push = dot(value, upper, ((0,), (0,))) + dot(value, lower, ((0,), (0,)))
            state = keep[:, at] * state + push
        return state

    lax.fori_loop(0, blocks // group, some, jnp.zeros((size, size), F32))


def within_kernel(query_ref, forget_ref, value_ref, tail_ref, mix_ref, high_ref, low_ref):
    heads, _, size = tail_ref.shape
    tails = [tail_ref[h].astype(F32) for h in range(heads)]
    free = jnp.concatenate([t[2:3] + t[1:2] + t[0:1] for t in tails], axis=1)
    leak, log_run = gate_terms(forget_ref[...], free)
    q_scaled = query_ref[...].astype(F32) * jnp.exp(log_run)
    k_scaled = leak * jnp.exp(-log_run)
    q_high, q_low = split(q_scaled)
    k_high, k_low = split(k_scaled)
    high_ref[...] = q_high
    low_ref[...] = q_low
    causal = tril(leak.shape[0])
    lanes = ((1,), (1,))
    for h in range(heads):
        at = slice(h * size, (h + 1) * size)
        scores = (
            dot(q_high[:, at], k_high[:, at], lanes)
            + dot(q_high[:, at], k_low[:, at], lanes)
            + dot(q_low[:, at], k_high[:, at], lanes)
        )
        s_high, s_low = split(jnp.where(causal, scores, 0.0))
        value = value_ref[:, at]
        mix_ref[:, at] = dot(s_high, value) + dot(s_low, value)


def finish_kernel(first, mix_ref, high_ref, low_ref, gate_ref, before_ref, gain_ref, out_ref):
    size = before_ref.shape[2]
    lanes = ((1,), (1,))
    for h in range(out_ref.shape[1] // size):
        to = slice(h * size, (h + 1) * size)
        at = slice((first + h) * size, (first + h + 1) * size)
        before = before_ref[first + h]
        mix = (
            mix_ref[:, at]
            + dot(high_ref[:, at], before, lanes)
            + dot(low_ref[:, at], before, lanes)
        )
        scale = lax.rsqrt(jnp.mean(mix * mix, axis=-1, keepdims=True) + NORM_EPS)
        normed = (mix * scale * gain_ref[...]).astype(BF16)
        u = gate_ref[:, at].astype(F32)
        out_ref[:, to] = (normed.astype(F32) * (u / (1.0 + jnp.exp(-u)))).astype(BF16)


def columns_kernel(place_ref, mine_a, mine_b, other_a, other_b, *refs):
    count = (len(refs) - 5) // 2
    w_refs, buffers = refs[:count], refs[count + 4 : 2 * count + 4]
    keep_ref, give_ref, mine_ref, other_ref = refs[count : count + 4]
    sems = refs[-1]
    copies = [
        pltpu.make_async_copy(w, buffer, sems.at[i])
        for i, (w, buffer) in enumerate(zip(w_refs, buffers))
    ]
    for copy in copies:
        copy.start()
    columns = w_refs[0].shape[1]
    depth = mine_ref.shape[1]
    half = mine_a.shape[1]
    mine_ref[:, :half], mine_ref[:, half:] = mine_a[...], mine_b[...]
    other_ref[:, :half], other_ref[:, half:] = other_a[...], other_b[...]
    n, done, totals = 0, 0, [0.0, 0.0]
    for i, (copy, buffer) in enumerate(zip(copies, buffers)):
        copy.wait()
        rows = buffer.shape[0]
        for k, src in enumerate((mine_ref, other_ref)):
            if rows == depth:
                totals[k] = dot(src[...], buffer[...])
            else:
                at = pl.multiple_of(place_ref[i] * rows, rows)
                totals[k] = totals[k] + dot(src[:, pl.ds(at, rows)], buffer[...])
        done += rows
        if done == depth:
            for total, dst in zip(totals, (keep_ref, give_ref)):
                dst[:, n * columns : (n + 1) * columns] = total.astype(BF16)
            n, done, totals = n + 1, 0, [0.0, 0.0]


def route_kernel(slot_ref, order_ref, *refs):
    *part_refs, residual_ref, gain_ref, outgoing_ref, hidden_ref, wide_ref, moe_ref, keep_ref = refs
    tokens, width = residual_ref.shape
    pieces = width // LANES
    columns = width // order_ref.shape[0]
    skew = moe_ref.shape[0] // pieces
    squares = jnp.zeros((tokens, 1), F32)
    parts = [
        ref[:, n * columns : (n + 1) * columns]
        for ref in part_refs
        for n in range(ref.shape[1] // columns)
    ]
    for n, part in enumerate(parts):
        at = pl.multiple_of(order_ref[n] * columns, columns)
        hidden = residual_ref[:, pl.ds(at, columns)].astype(F32) + part.astype(F32)
        hidden = hidden.astype(BF16).astype(F32)
        wide_ref[:, pl.ds(at, columns)] = hidden
        squares = squares + jnp.sum(hidden * hidden, axis=-1, keepdims=True)
    scale = lax.rsqrt(squares / width + NORM_EPS)
    for c in range(pieces):
        part = wide_ref[:, c * LANES : (c + 1) * LANES]
        keep_ref[c * skew : c * skew + tokens, :] = part
        gain = gain_ref[:, c * LANES : (c + 1) * LANES]
        moe_ref[c * skew : c * skew + tokens, :] = part * scale * gain

    def keep_row(t, _):
        hidden_ref[t] = keep_ref[pl.ds(t, pieces, stride=skew), :].astype(BF16)
        return 0

    lax.fori_loop(0, tokens, keep_row, 0, unroll=4)

    def fill_slot(s, _):
        outgoing_ref[s] = moe_ref[pl.ds(slot_ref[s], pieces, stride=skew), :].astype(BF16)
        return 0

    lax.fori_loop(0, outgoing_ref.shape[0], fill_slot, 0, unroll=8)


def expert_kernel(rows_ref, gate_ref, up_ref, down_ref, out_ref, wide_ref, x_ref):
    pieces = rows_ref.shape[1]
    rows = x_ref.shape[0]
    skew = wide_ref.shape[0] // pieces

    def some(i, _):
        first = i * rows

        def spread(r, _):
            wide_ref[pl.ds(r, pieces, stride=skew), :] = rows_ref[first + r].astype(F32)
            return 0

        lax.fori_loop(0, rows, spread, 0, unroll=8)
        for c in range(pieces):
            x_ref[:, c * LANES : (c + 1) * LANES] = wide_ref[
                c * skew : c * skew + rows, :
            ].astype(BF16)
        gate = dot(x_ref[...], gate_ref[...])
        up = dot(x_ref[...], up_ref[...])
        act = (gate / (1.0 + jnp.exp(-gate)) * up).astype(BF16)
        step = 4
        for c in range(0, pieces, step):
            part = dot(act, down_ref[:, c * LANES : (c + step) * LANES])
            for k in range(step):
                wide_ref[(c + k) * skew : (c + k) * skew + rows, :] = part[
                    :, k * LANES : (k + 1) * LANES
                ]

        def gather(r, _):
            out_ref[first + r] = wide_ref[pl.ds(r, pieces, stride=skew), :].astype(BF16)
            return 0

        lax.fori_loop(0, rows, gather, 0, unroll=8)
        return 0

    lax.fori_loop(0, rows_ref.shape[0] // rows, some, 0)


def combine_kernel(target_ref, weight_ref, back_ref, hidden_ref, out_ref, wide_ref):
    tokens, pieces, _ = hidden_ref.shape
    skew = wide_ref.shape[0] // pieces
    top = target_ref.shape[0] // tokens

    def one(t, _):
        total = jnp.zeros((pieces, LANES), F32)
        for j in range(top):
            i = t * top + j
            total = total + weight_ref[i] * back_ref[target_ref[i]].astype(F32)
        wide_ref[pl.ds(t, pieces, stride=skew), :] = hidden_ref[t].astype(F32) + total
        return 0

    lax.fori_loop(0, tokens, one, 0, unroll=4)
    for c in range(pieces):
        out_ref[:, c * LANES : (c + 1) * LANES] = wide_ref[
            c * skew : c * skew + tokens, :
        ].astype(BF16)


def whole(shape, space=None):
    if space is None:
        return pl.BlockSpec(shape, lambda *_: (0,) * len(shape))
    return pl.BlockSpec(memory_space=space)


def cost(flops, moved):
    return pl.CostEstimate(flops=int(flops), bytes_accessed=int(moved), transcendentals=0)


def slots_of(chosen, experts, capacity, tokens, top_count):
    matches = (chosen[:, None] == jnp.arange(experts, dtype=jnp.int32)[None, :]).astype(jnp.int32)
    rank_in = jnp.sum((jnp.cumsum(matches, axis=0) - 1) * matches, axis=1)
    target = chosen * capacity + rank_in
    owners = jnp.arange(tokens * top_count, dtype=jnp.int32) // top_count
    slot_owner = jnp.zeros((experts * capacity,), jnp.int32).at[target].set(owners)
    return target, slot_owner


def local(
    queries,
    forget_pre,
    values,
    out_gate,
    lower_bound,
    head_gain,
    residual,
    out_weight,
    ffn_gain,
    routing,
    route_weight,
    expert_gate,
    expert_up,
    expert_down,
):
    tokens = queries.shape[1]
    channels = queries.shape[2]
    size = head_gain.shape[0]
    heads = channels // size
    width = residual.shape[2]
    pieces = width // LANES
    top_count = routing.shape[2]
    span = lax.axis_size("sp") * lax.axis_size("dp")
    experts = expert_gate.shape[0] * span
    slots = experts * CAPACITY

    ring = lax.axis_size("dp")
    turn = 4
    at_z, at_x = lax.axis_index("sp") // turn, lax.axis_index("sp") % turn
    along = (at_x + 2 * at_z) % turn
    across = [(d, d ^ 1) for d in range(ring)]

    def hop(x, chips):
        return lax.ppermute(x, "dp", [(d, (d + 2 * chips) % ring) for d in range(ring)])

    def pass_on(x, steps):
        moves = [(s, s // turn * turn + (s + steps) % turn) for s in range(lax.axis_size("sp"))]
        return lax.ppermute(x, "sp", moves)

    def pass_up(x):
        rows = lax.axis_size("sp")
        return lax.ppermute(x, "sp", [(s, (s + turn) % rows) for s in range(rows)])

    quarter = channels // turn
    far = hop(lax.dynamic_slice_in_dim(out_weight, along * quarter, quarter), 2)
    before_block = hop(out_weight, 1)
    after_block = hop(out_weight, -1)

    def swap(x):
        return lax.ppermute(x, "dp", across)

    in_vmem = whole(None, pltpu.VMEM)
    q = queries.reshape(tokens, channels)
    f = forget_pre.reshape(tokens, channels)
    v = values.reshape(tokens, channels)
    g = out_gate.reshape(tokens, channels)
    bound = lower_bound.reshape(1, size)
    message = 2 * tokens + MSG_PAD
    pair = pl.pallas_call(
        pair_kernel,
        in_specs=[in_vmem] * 3,
        out_specs=in_vmem,
        out_shape=jax.ShapeDtypeStruct((heads, message, size), BF16),
        cost_estimate=cost(1e6, 2e6),
        compiler_params=pltpu.CompilerParams(vmem_limit_bytes=60 * 2**20),
        name="pair",
    )(f, v, bound)
    arrived = lax.all_to_all(pair, "sp", split_axis=0, concat_axis=0, tiled=True)
    far_parts = (far, pass_on(far, 1), pass_on(far, -1), pass_up(far))
    before = pl.pallas_call(
        state_kernel,
        in_specs=[in_vmem, in_vmem],
        out_specs=in_vmem,
        out_shape=jax.ShapeDtypeStruct((arrived.shape[0], size, size), BF16),
        cost_estimate=cost(1e9, 2e6),
        compiler_params=pltpu.CompilerParams(vmem_limit_bytes=12 * 2**20),
        name="state",
    )(arrived, bound)
    before = lax.all_to_all(before, "sp", split_axis=0, concat_axis=0, tiled=True)
    target, slot_owner = slots_of(
        routing.reshape(tokens * top_count), experts, CAPACITY, tokens, top_count
    )
    per_step = 4
    head_block = pl.BlockSpec((tokens, per_step * size), lambda h: (0, h))
    mix_shape = jax.ShapeDtypeStruct((tokens, channels), F32)
    q_shape = jax.ShapeDtypeStruct((tokens, channels), BF16)
    mix, q_high, q_low = pl.pallas_call(
        within_kernel,
        grid=(heads // per_step,),
        in_specs=[head_block] * 3
        + [pl.BlockSpec((per_step, MSG_PAD, size), lambda h: (h, 2 * tokens // MSG_PAD, 0))],
        out_specs=[head_block] * 3,
        out_shape=[mix_shape, q_shape, q_shape],
        cost_estimate=cost(2e9, 3e6),
        compiler_params=pltpu.CompilerParams(vmem_limit_bytes=60 * 2**20),
        name="within",
    )(q, f, v, arrived)

    def finish(first, count):
        return pl.pallas_call(
            functools.partial(finish_kernel, first),
            in_specs=[in_vmem] * 6,
            out_specs=in_vmem,
            out_shape=jax.ShapeDtypeStruct((tokens, count * size), BF16),
            cost_estimate=cost(6e8, 2e6),
            compiler_params=pltpu.CompilerParams(vmem_limit_bytes=12 * 2**20),
            name="finish",
        )(mix, q_high, q_low, g, before, head_gain.reshape(1, size))

    weights = route_weight.reshape(tokens * top_count)
    gated_a = finish(0, heads // 2)
    other_a = swap(gated_a)
    gated_b = finish(heads // 2, heads // 2)
    gated_b, slot_owner, target, weights = lax.optimization_barrier(
        (gated_b, slot_owner, target, weights)
    )
    other_b = swap(gated_b)
    columns = out_weight.shape[1]

    def project(limit, *parts):
        wide = sum(p.shape[0] for p in parts) // channels * columns
        shape = jax.ShapeDtypeStruct((tokens, wide), BF16)
        keep, give = pl.pallas_call(
            columns_kernel,
            in_specs=[whole(None, pltpu.SMEM)]
            + [in_vmem] * 4
            + [whole(None, pl.ANY)] * len(parts),
            out_specs=[in_vmem] * 2,
            out_shape=[shape] * 2,
            scratch_shapes=[pltpu.VMEM((tokens, channels), BF16)] * 2
            + [pltpu.VMEM(p.shape, BF16) for p in parts]
            + [pltpu.SemaphoreType.DMA((len(parts),))],
            cost_estimate=cost(4 * tokens * channels * wide, 2 * channels * wide),
            compiler_params=pltpu.CompilerParams(vmem_limit_bytes=limit * 2**20),
        )(place, gated_a, gated_b, other_a, other_b, *parts)
        return keep, swap(give)

    place = jnp.stack([(along + turn - shift) % turn for shift in (0, 1, turn - 1, 2)])
    place = place.astype(jnp.int32)
    early = project(10, *far_parts, out_weight)
    late = project(10, before_block, after_block)
    chip, core = lax.axis_index("dp") // 2, lax.axis_index("dp") % 2
    order = jnp.stack(
        [
            (chip + hop) % (ring // 2) * 2 + parity
            for hops in ((2, 0), (ring // 2 - 1, 1))
            for parity in (core, 1 - core)
            for hop in hops
        ]
    ).astype(jnp.int32)
    skew = tokens + 1
    outgoing, hidden = pl.pallas_call(
        route_kernel,
        in_specs=[whole(None, pltpu.SMEM)] * 2 + [in_vmem] * 6,
        out_specs=[in_vmem, in_vmem],
        out_shape=[
            jax.ShapeDtypeStruct((slots, pieces, LANES), BF16),
            jax.ShapeDtypeStruct((tokens, pieces, LANES), BF16),
        ],
        scratch_shapes=[
            pltpu.VMEM((tokens, width), F32),
            pltpu.VMEM((skew * pieces + 8, LANES), F32),
            pltpu.VMEM((skew * pieces + 8, LANES), F32),
        ],
        cost_estimate=cost(4e7, 12e6),
        compiler_params=pltpu.CompilerParams(vmem_limit_bytes=24 * 2**20),
        name="route",
    )(
        slot_owner,
        order,
        *early,
        *late,
        residual.reshape(tokens, width),
        ffn_gain.reshape(1, width),
    )

    exchange = functools.partial(
        lax.all_to_all, axis_name=("sp", "dp"), split_axis=0, concat_axis=0, tiled=True
    )
    chunk = (span, CAPACITY * pieces, LANES)
    rows_in = exchange(outgoing.reshape(chunk)).reshape(slots, pieces, LANES)
    hidden_units = expert_gate.shape[2]
    rows = slots // 2
    results = pl.pallas_call(
        expert_kernel,
        in_specs=[in_vmem] * 4,
        out_specs=in_vmem,
        out_shape=jax.ShapeDtypeStruct((slots, pieces, LANES), BF16),
        scratch_shapes=[
            pltpu.VMEM(((rows + 1) * pieces + 8, LANES), F32),
            pltpu.VMEM((rows, width), BF16),
        ],
        cost_estimate=cost(8e9, 24e6),
        compiler_params=pltpu.CompilerParams(vmem_limit_bytes=20 * 2**20),
        name="expert",
    )(
        rows_in,
        expert_gate.reshape(width, hidden_units),
        expert_up.reshape(width, hidden_units),
        expert_down.reshape(hidden_units, width),
    )
    back = exchange(results.reshape(chunk)).reshape(slots, pieces, LANES)
    out = pl.pallas_call(
        combine_kernel,
        in_specs=[
            whole(None, pltpu.SMEM),
            whole(None, pltpu.SMEM),
            whole(None, pltpu.VMEM),
            whole(None, pltpu.VMEM),
        ],
        out_specs=whole(None, pltpu.VMEM),
        out_shape=jax.ShapeDtypeStruct((tokens, width), BF16),
        scratch_shapes=[pltpu.VMEM((skew * pieces + 8, LANES), F32)],
        cost_estimate=cost(4e8, 8e6),
        compiler_params=pltpu.CompilerParams(vmem_limit_bytes=16 * 2**20),
        name="combine",
    )(target, weights, back, hidden)
    return out.reshape(1, tokens, width)


def solution(mesh):
    in_specs = (
        P("dp", "sp", None),
        P("dp", "sp", None),
        P("dp", "sp", None),
        P("dp", "sp", None),
        P("sp"),
        P(),
        P("dp", "sp", None),
        P(None, "dp"),
        P(),
        P("dp", "sp", None),
        P("dp", "sp", None),
        P(("sp", "dp"), None, None),
        P(("sp", "dp"), None, None),
        P(("sp", "dp"), None, None),
    )
    out_specs = P("dp", "sp", None)
    return jax.shard_map(local, mesh=mesh, in_specs=in_specs, out_specs=out_specs, check_vma=False)
```
